512 devices in a mesh: ep: 32 (over z, x), tp: 16 (over y, core).
Axes of the slice: x: 4, y: 8, z: 8, core: 2. Of those that a mesh axis runs over, the one named last changes fastest.
Arguments:
- mixer_input_rows: bfloat16 [4096, 2048], P('ep'), may hold values from -6 to 6
- mix_gain: float32 [2048], replicated, may hold values from 0.1 to 1.9
- w_recept: bfloat16 [2048, 1024], P(None, 'tp'), may hold values from -0.125 to 0.125
- w_key: bfloat16 [2048, 1024], P(None, 'tp'), may hold values from -0.125 to 0.125
- w_value: bfloat16 [2048, 1024], P(None, 'tp'), may hold values from -0.125 to 0.125
- lowered_map_factor: bfloat16 [2048, 64], replicated, may hold values from -0.125 to 0.125
- decay_up: bfloat16 [64, 1024], P(None, 'tp'), may hold values from -0.75 to 0.75
- rate_up: bfloat16 [64, 1024], P(None, 'tp'), may hold values from -0.75 to 0.75
- decay_base: float32 [1024], P('tp'), may hold values from -13 to -2
- rate_base: float32 [1024], P('tp'), may hold values from -9 to 1
- decay_shift: float32 [4096, 16], P('ep', 'tp'), may hold values from -0.7 to 0, as said below
- out_gain: float32 [1024], P('tp'), may hold values from 0.1 to 1.9
- w_output: bfloat16 [1024, 2048], P('tp'), may hold values from -0.1875 to 0.1875
- moe_rows: bfloat16 [4096, 2048], P('ep'), may hold values from -6 to 6
- moe_gain: float32 [2048], replicated, may hold values from 0.1 to 1.9
- routes: int32 [4096, 2], P('ep'), may hold values from 0 to 31, all different within a row; in each aligned block of 128 rows (0 to 127, 128 to 255, ...) at most 16 rows name the same one
- route_weight: float32 [4096, 2], P('ep'), may hold values from 0.1 to 1
- exp_gate: bfloat16 [32, 2048, 4096], P('ep', None, 'tp'), may hold values from -0.125 to 0.125
- exp_up: bfloat16 [32, 2048, 4096], P('ep', None, 'tp'), may hold values from -0.125 to 0.125
- exp_down: bfloat16 [32, 4096, 2048], P('ep', 'tp'), may hold values from -0.125 to 0.125
Outputs:
- mix_out: bfloat16 [4096, 2048], P(('ep', 'tp'))
- moe_out: bfloat16 [4096, 2048], P('ep', 'tp')
The draws below stay inside these ranges and needn't reach their ends.
Inputs may be any that keep to these rules, and one draw needn't show every extreme that they name: `routes`: in each aligned block of 128 rows no expert is named more than 16 times, and in some block one expert is named exactly 16 times; the two entries of a row differ. `decay_shift`: at most zero.
All inputs are finite; a program needn't handle non-finite values.
Results may differ from the reference program's by a relative error of at most 0.02.
Values may be sent and summed in bfloat16 or wider, within the bound.
No kernel may reach another device: no remote copies, remote signals or barrier semaphores. Data moves between devices by JAX's collectives and lax.ppermute only.
A program may use at most 64 MiB of HBM per device.

```python
import math
from functools import partial
import jax
import jax.numpy as jnp
import numpy as np
from jax import lax

D = 2048
HEADS = 16
HEAD_DIM = 64
RANK = 64
EXP_HIDDEN = 4096
MIX_TOK = 128
MOE_TOK = 128
CHANNELS = 1024
SEQ_ITEMS_FIRST = 4096
MOE_TOKENS = 4096
EXPERTS = 32
SLOTS = 16
N_EP = 32
N_TP = 16


def head_groups(key):
    fast_count = max(1, HEADS // 4)
    middle_count = max(1, HEADS // 4)
    shuffled = jax.random.permutation(jax.random.fold_in(key, 101), HEADS)
    group_ids = jnp.where(shuffled < fast_count, 0, jnp.where(shuffled < fast_count + middle_count, 1, 2))
    return jnp.repeat(group_ids, HEAD_DIM)


def draw_decay_base(key, part):
    group_ids = head_groups(key)
    spread = jax.random.uniform(jax.random.fold_in(key, 1), (CHANNELS,), jnp.float32)
    return jnp.where(group_ids == 0, -3.5 + 1.5 * spread, -13.0 + 2.5 * spread)


def draw_rate_base(key, part):
    group_ids = head_groups(key)
    spread = jax.random.uniform(jax.random.fold_in(key, 2), (CHANNELS,), jnp.float32)
    fast_level = -1.5 + 2.5 * spread
    middle_level = -4.0 + 3.0 * spread
    slow_level = -9.0 + 2.0 * spread
    return jnp.where(group_ids == 0, fast_level, jnp.where(group_ids == 1, middle_level, slow_level))


def draw_decay_shift(key, part):
    low_level = 2e-05
    high_level = 0.0002
    blocks = SEQ_ITEMS_FIRST // MIX_TOK
    level_draw = jax.random.uniform(jax.random.fold_in(key, 3), (blocks, HEADS), jnp.float32)
    hierarchy_tiers = jnp.exp(jnp.log(low_level) + (jnp.log(high_level) - jnp.log(low_level)) * level_draw)
    hierarchy_tiers = jnp.repeat(hierarchy_tiers, MIX_TOK, axis=0)
    spike_offsets = jax.random.randint(jax.random.fold_in(key, 5), (3,), 0, SEQ_ITEMS_FIRST)
    entry_offsets = jnp.arange(SEQ_ITEMS_FIRST)
    spike_entry_tile = jnp.any(entry_offsets[:, None] == spike_offsets[None, :], axis=1)
    prefix_heights = jax.random.uniform(jax.random.fold_in(key, 7), (SEQ_ITEMS_FIRST, HEADS), jnp.float32, 0.22, 0.69)
    return -hierarchy_tiers - jnp.where(spike_entry_tile[:, None], prefix_heights, 0.0)


def spiked(result, own_key, source, target, blocks, factor):
    def block_of(dim):
        return (jnp.arange(result.shape[dim]) // (result.shape[dim] // blocks)).reshape((-1,) + (1,) * (result.ndim - 1 - dim))

    first = jax.random.permutation(own_key, blocks)[block_of(target)]
    far = (block_of(target) + blocks // 2) % blocks
    return jnp.where((block_of(source) == first) | (block_of(source) == far), factor * result, result)


def shard_levels(stream_key, extent, shards, smallest, top_value):
    gain, own = 1.0, jax.random.fold_in(stream_key, 6)
    for dim, blocks in shards:
        steps = jnp.exp(jax.random.uniform(jax.random.fold_in(own, dim), (blocks,), jnp.float32, smallest / len(shards), top_value / len(shards)))
        gain = gain * jnp.repeat(steps, extent[dim] // blocks).reshape([-1 if axis == dim else 1 for axis in range(len(extent))])
    return gain


def deal_out(key, own, number, rows, amount, top, most, skew):
    order = jax.random.permutation(key, amount)
    crowded, usual = shares(amount, rows * top, most, skew, True), shares(amount, rows * top, most, skew, False)
    places = jnp.arange(amount)

    def named(sizes, rotation):
        used = int((sizes > 0).sum())
        fixed = max(1, used // 4)
        moved = fixed + (places - fixed + rotation * (used - fixed)) % max(1, amount - fixed)
        return jnp.zeros((amount,), jnp.int32).at[order[jnp.where(places < fixed, places, moved)]].set(jnp.asarray(sizes, jnp.int32))

    sizes = jnp.where(number % 4 == 0, named(crowded, number // 4), named(usual, number - number // 4 - 1))
    mixed = jax.random.permutation(jax.random.fold_in(own, 3), amount)
    donor, sink = mixed[0:amount // 2 * 2:2], mixed[1:amount // 2 * 2:2]
    room = jnp.minimum(sizes[donor] - 1, most - sizes[sink]) // 2
    room = jnp.where((donor == order[0]) | (sink == order[0]) | (sizes[sink] == 0), 0, jnp.maximum(room, 0))
    moved = jax.random.randint(jax.random.fold_in(own, 4), (amount // 2,), 0, 1 << 20) % (room + 1)
    sizes = sizes.at[donor].add(-moved).at[sink].add(moved)
    labels = jnp.searchsorted(jnp.cumsum(sizes), jnp.arange(rows * top), side="right").astype(jnp.int32)
    grid = labels.reshape(top, rows).T
    grid = grid[jax.random.permutation(jax.random.fold_in(own, 1), rows)]
    rotation = jax.random.randint(jax.random.fold_in(own, 2), (rows, 1), 0, top)
    return jnp.take_along_axis(grid, (jnp.arange(top)[None, :] + rotation) % top, axis=1)


def shares(count, total, most, skew, full):
    loads = [(1 << 20) // math.isqrt(grade ** skew) + 1 for grade in range(1, count + 1)]
    largest = most if full else min(most, max(-(-total // count), total * loads[0] // sum(loads)))
    least = 1 if total - largest >= count - 1 else 0
    given, rest = [largest] + [least] * (count - 1), total - largest - least * (count - 1)
    while rest > 0:
        free = [i for i in range(1, count) if given[i] < largest] or [i for i in range(1, count) if given[i] < most]
        whole, budget = sum([loads[i] for i in free]), rest
        for i in free:
            more = min(most - given[i], max(1, budget * loads[i] // whole), rest)
            given[i] = given[i] + more
            rest = rest - more
    return np.array(given)


def noise(own_key, dims, width, reach, cuts=(), kind=jnp.bfloat16):
    array = jax.random.normal(own_key, dims, jnp.float32) * width
    if len(cuts) > 0:
        array = shard_levels(own_key, dims, cuts, -0.22, 0.18) * array
    return jnp.clip(array, min=-reach, max=reach).astype(kind)


def gaussian_with(stream_key, shape, width, reach, shards, heavy, held_as=jnp.bfloat16):
    result = width * jax.random.normal(stream_key, shape, jnp.float32)
    if shards:
        result = result * shard_levels(stream_key, shape, shards, -0.22, 0.18)
    return jnp.clip(spiked(result, jax.random.fold_in(stream_key, 3), *heavy), -reach, reach).astype(held_as)


def setup_inputs(seed: int = 0) -> dict:
    arg_keys = jax.random.split(jax.random.key(seed), 21)
    mixer_input_rows = noise(arg_keys[0], (SEQ_ITEMS_FIRST, D), 1.0, 6.0, ((0, 32),))
    mix_gain = jnp.clip(1.0 + 0.18 * jax.random.normal(arg_keys[1], (D,), jnp.float32), 0.1, 1.9)
    w_recept = noise(arg_keys[2], (D, CHANNELS), D ** -0.5, 0.125, ((1, 16),))
    w_key = noise(arg_keys[3], (D, CHANNELS), D ** -0.5, 0.125, ((1, 16),))
    w_value = noise(arg_keys[4], (D, CHANNELS), D ** -0.5, 0.125, ((1, 16),))
    lowered_map_factor = noise(arg_keys[5], (D, RANK), D ** -0.5, 0.125)
    decay_up = noise(arg_keys[6], (RANK, CHANNELS), RANK ** -0.5, 0.75, ((1, 16),))
    rate_up = noise(arg_keys[7], (RANK, CHANNELS), RANK ** -0.5, 0.75, ((1, 16),))
    decay_base = draw_decay_base(jax.random.fold_in(arg_keys[20], 71), 0)
    rate_base = draw_rate_base(jax.random.fold_in(arg_keys[20], 71), 0)
    decay_shift = draw_decay_shift(jax.random.fold_in(arg_keys[20], 71), 0)
    out_gain = jnp.clip(1.0 + 0.18 * jax.random.normal(arg_keys[11], (CHANNELS,), jnp.float32), 0.1, 1.9)
    w_output = noise(arg_keys[12], (CHANNELS, D), CHANNELS ** -0.5, 0.1875, ((0, 16),))
    moe_rows = noise(arg_keys[13], (MOE_TOKENS, D), 1.0, 6.0, ((0, 32),))
    moe_gain = jnp.clip(1.0 + 0.18 * jax.random.normal(arg_keys[14], (D,), jnp.float32), 0.1, 1.9)
    routes_keys = jax.random.split(jax.random.fold_in(arg_keys[15], 1), MOE_TOKENS // MOE_TOK)
    routes_turns = jax.random.permutation(jax.random.fold_in(arg_keys[15], 3), MOE_TOKENS // MOE_TOK)
    routes = jax.vmap(lambda own, number: deal_out(jax.random.fold_in(arg_keys[15], 2), own, number, MOE_TOK, EXPERTS, 2, SLOTS, 2))(routes_keys, routes_turns).reshape((MOE_TOKENS, 2))
    route_weight = jnp.clip(0.1 + 0.9 * jax.random.uniform(arg_keys[16], (MOE_TOKENS, 2), jnp.float32) ** shard_levels(arg_keys[16], (MOE_TOKENS, 2), ((0, 32),), -0.2, 0.2), 0.1, 1.0)
    exp_gate = noise(arg_keys[17], (EXPERTS, D, EXP_HIDDEN), D ** -0.5, 0.125, ((0, 32), (2, 16)))
    exp_up = noise(arg_keys[18], (EXPERTS, D, EXP_HIDDEN), D ** -0.5, 0.125, ((0, 32), (2, 16)))
    exp_down = gaussian_with(arg_keys[19], (EXPERTS, EXP_HIDDEN, D), EXP_HIDDEN ** -0.5, 0.125, ((0, 32), (1, 16)), (1, 2, 16, 2.0))
    return {"mixer_input_rows": mixer_input_rows, "mix_gain": mix_gain, "w_recept": w_recept, "w_key": w_key, "w_value": w_value, "lowered_map_factor": lowered_map_factor, "decay_up": decay_up, "rate_up": rate_up, "decay_base": decay_base, "rate_base": rate_base, "decay_shift": decay_shift, "out_gain": out_gain, "w_output": w_output, "moe_rows": moe_rows, "moe_gain": moe_gain, "routes": routes, "route_weight": route_weight, "exp_gate": exp_gate, "exp_up": exp_up, "exp_down": exp_down}


HIGHEST = lax.Precision.HIGHEST
DECAY_SCALE = math.exp(-0.5)

def row_norm(row_block, gain_vector):
    entries = row_block.astype(jnp.float32)
    factor = lax.rsqrt(lax.optimization_barrier(jnp.mean(entries * entries, axis=-1, keepdims=True)) + 1e-06)
    return (entries * factor * gain_vector.astype(jnp.float32)).astype(jnp.bfloat16)

def block_sum(left_side, right_side, blocks):
    block_width = left_side.shape[1] // blocks

    def accumulate(running, position):
        start_at = (position * block_width).astype(jnp.int32)
        left_part = lax.dynamic_slice_in_dim(left_side, start_at, block_width, 1)
        right_part = lax.dynamic_slice_in_dim(right_side, start_at, block_width, 0)
        product = jnp.dot(left_part, right_part, preferred_element_type=jnp.float32)
        rounded = lax.optimization_barrier(product.astype(jnp.bfloat16))
        return (running + rounded.astype(jnp.float32), None)
    start_sum = jnp.zeros((left_side.shape[0], right_side.shape[1]), jnp.float32)
    running, _ = lax.scan(accumulate, start_sum, jnp.arange(blocks, dtype=jnp.int32))
    return running.astype(jnp.bfloat16)

def route_tables(route_rows, weight_rows, expert_count, slot_count):
    route_list = route_rows.reshape(-1)
    onehot = (route_list[:, None] == jnp.arange(expert_count, dtype=jnp.int32)[None, :]).astype(jnp.int32)
    slot_index = lax.optimization_barrier(jnp.sum((jnp.cumsum(onehot, axis=0) - onehot) * onehot, axis=1))
    target = (route_list * slot_count + slot_index).reshape(route_rows.shape)
    columns = jnp.arange(expert_count * slot_count, dtype=jnp.int32)
    matches = target[:, :, None] == columns[None, None, :]
    placing = lax.optimization_barrier(jnp.sum(matches.astype(jnp.int32), axis=1)).astype(jnp.bfloat16)
    rounded = weight_rows.astype(jnp.bfloat16)
    weighing = lax.optimization_barrier(jnp.sum(jnp.where(matches, rounded[:, :, None], jnp.zeros((), jnp.bfloat16)), axis=1))
    return (placing, weighing.astype(jnp.bfloat16))

def mixer(mixer_input_rows, mix_gain, w_recept, w_key, w_value, lowered_map_factor, decay_up, rate_up, decay_base, rate_base, decay_shift, out_gain, w_output):
    normed_input = row_norm(mixer_input_rows, mix_gain)

    def heads_of(weight):
        product = jnp.dot(normed_input, weight, preferred_element_type=jnp.float32)
        rounded = lax.optimization_barrier(product.astype(jnp.bfloat16))
        return rounded.astype(jnp.float32).reshape(SEQ_ITEMS_FIRST, HEADS, HEAD_DIM)
    recept_heads = heads_of(w_recept)
    key_heads = heads_of(w_key)
    value_heads = heads_of(w_value)
    lowrank = jnp.tanh(jnp.dot(normed_input, lowered_map_factor, preferred_element_type=jnp.float32)).astype(jnp.bfloat16)
    decay_pre = decay_base + jnp.dot(lowrank, decay_up, preferred_element_type=jnp.float32)
    log_decay = -DECAY_SCALE * jax.nn.sigmoid(decay_pre) + jnp.repeat(decay_shift, HEAD_DIM, axis=1)
    learn_rate = jax.nn.sigmoid(rate_base + jnp.dot(lowrank, rate_up, preferred_element_type=jnp.float32))
    decay_rate = jnp.exp(log_decay).reshape(SEQ_ITEMS_FIRST, HEADS, HEAD_DIM)
    learn_rate = learn_rate.reshape(SEQ_ITEMS_FIRST, HEADS, HEAD_DIM)
    unit_key = key_heads * lax.rsqrt(lax.optimization_barrier(jnp.sum(key_heads * key_heads, axis=-1, keepdims=True)) + 1e-06)

    def advance(memory, inputs):
        decay_row, unit_row, learn_row, key_row, value_row, recept_row = inputs
        along_key = jnp.einsum('hij,hj->hi', memory, unit_row, precision=HIGHEST)
        memory = memory * decay_row[:, None, :] - along_key[:, :, None] * (unit_row * learn_row)[:, None, :] + value_row[:, :, None] * key_row[:, None, :]
        return (memory, jnp.einsum('hij,hj->hi', memory, recept_row, precision=HIGHEST))
    start_state = jnp.zeros((HEADS, HEAD_DIM, HEAD_DIM), jnp.float32)
    sequence = (decay_rate, unit_key, learn_rate, key_heads, value_heads, recept_heads)
    _, forward_out = lax.scan(advance, start_state, sequence)
    _, backward_out = lax.scan(advance, start_state, sequence, reverse=True)
    mixed_out = forward_out + backward_out
    centre = mixed_out - lax.optimization_barrier(jnp.mean(mixed_out, axis=-1, keepdims=True))
    scaled = centre * lax.rsqrt(lax.optimization_barrier(jnp.mean(centre * centre, axis=-1, keepdims=True)) + 1e-05)
    grouped = (scaled * out_gain.reshape(HEADS, HEAD_DIM)).astype(jnp.bfloat16).reshape(SEQ_ITEMS_FIRST, CHANNELS)
    return block_sum(grouped, w_output, N_TP)

def fill_slots(placing_group, rows_group):
    product = lax.dot_general(placing_group, rows_group, (((0,), (0,)), ((), ())), preferred_element_type=jnp.float32)
    return product.astype(jnp.bfloat16)

def combine_group(weighing_group, result_group):
    return jnp.dot(weighing_group, result_group, preferred_element_type=jnp.float32).astype(jnp.bfloat16)

def experts_layer(moe_rows, moe_gain, routes, route_weight, exp_gate, exp_up, exp_down):
    moe_normed = row_norm(moe_rows, moe_gain)
    group_rows = moe_normed.reshape(N_EP, MOE_TOK, D)
    group_routes = routes.reshape(N_EP, MOE_TOK, 2)
    group_weights = route_weight.reshape(N_EP, MOE_TOK, 2)
    tables = jax.vmap(partial(route_tables, expert_count=EXPERTS, slot_count=SLOTS))
    placing, weighing = tables(group_routes, group_weights)
    buffers = jax.vmap(fill_slots)(placing, group_rows).reshape(N_EP, EXPERTS, SLOTS, D)

    def run_expert(expert_index):
        slot_rows = lax.dynamic_index_in_dim(buffers, expert_index, 1, keepdims=False).reshape(N_EP * SLOTS, D)
        gate_weight = lax.dynamic_index_in_dim(exp_gate, expert_index, 0, keepdims=False)
        up_weight = lax.dynamic_index_in_dim(exp_up, expert_index, 0, keepdims=False)
        down_weight = lax.dynamic_index_in_dim(exp_down, expert_index, 0, keepdims=False)
        gate_part = jnp.dot(slot_rows, gate_weight, preferred_element_type=jnp.float32)
        up_part = jnp.dot(slot_rows, up_weight, preferred_element_type=jnp.float32)
        hidden = (jax.nn.silu(gate_part) * up_part).astype(jnp.bfloat16)
        return block_sum(hidden, down_weight, N_TP)
    results = lax.map(run_expert, jnp.arange(EXPERTS, dtype=jnp.int32))
    results = jnp.swapaxes(results.reshape(EXPERTS, N_EP, SLOTS, D), 0, 1).reshape(N_EP, EXPERTS * SLOTS, D)
    combined = jax.vmap(combine_group)(weighing, results)
    return combined.reshape(MOE_TOKENS, D)

def reference(mixer_input_rows, mix_gain, w_recept, w_key, w_value, lowered_map_factor, decay_up, rate_up, decay_base, rate_base, decay_shift, out_gain, w_output, moe_rows, moe_gain, routes, route_weight, exp_gate, exp_up, exp_down):
    mix_out = mixer(mixer_input_rows, mix_gain, w_recept, w_key, w_value, lowered_map_factor, decay_up, rate_up, decay_base, rate_base, decay_shift, out_gain, w_output)
    moe_out = experts_layer(moe_rows, moe_gain, routes, route_weight, exp_gate, exp_up, exp_down)
    return (mix_out, moe_out)
```

```python
import functools
import math

import jax
import jax.numpy as jnp
from jax import lax
from jax.experimental import pallas as pl
from jax.experimental.pallas import tpu as pltpu
from jax.sharding import PartitionSpec as P


DECAY_SCALE = math.exp(-0.5)
HIGH = lax.Precision.HIGHEST
F32 = jnp.float32
BF16 = jnp.bfloat16
ROW = 4


def mm(a, b, precision=HIGH):
    return lax.dot_general(
        a, b, (((1,), (0,)), ((), ())), precision=precision, preferred_element_type=F32
    )


def mm_nt(a, b, precision=HIGH):
    return lax.dot_general(
        a, b, (((1,), (1,)), ((), ())), precision=precision, preferred_element_type=F32
    )


def mm_tn(a, b, precision=HIGH):
    return lax.dot_general(
        a, b, (((0,), (0,)), ((), ())), precision=precision, preferred_element_type=F32
    )


def norm_rows(rows, gain):
    entries = rows.astype(F32)
    factor = lax.rsqrt(jnp.mean(entries * entries, axis=-1, keepdims=True) + 1e-06)
    return (entries * factor * gain).astype(BF16)


def block_totals(log_decay, unit, rate, key, value, recept, reverse):
    tokens, width = log_decay.shape
    half = tokens // 2
    i = lax.broadcasted_iota(jnp.int32, (tokens, tokens), 0)
    j = lax.broadcasted_iota(jnp.int32, (tokens, tokens), 1)
    upto = (j >= i) if reverse else (j <= i)
    before = (j > i) if reverse else (j < i)
    same = (i // half) == (j // half)
    cum = mm(upto.astype(F32), log_decay)
    exc = cum - log_decay
    row = lax.broadcasted_iota(jnp.int32, (tokens, width), 0)
    if reverse:
        total = cum[:1]
        edge = cum[half : half + 1]
        first = row >= half
        mid_low, mid_high = (half // 2, half + half // 2)
    else:
        total = cum[tokens - 1 :]
        edge = cum[half - 1 : half]
        first = row < half
        mid_low, mid_high = (half // 2 - 1, half + half // 2 - 1)
    ref = jnp.where(row < half, cum[mid_low : mid_low + 1], cum[mid_high : mid_high + 1])
    learned = unit * rate
    down = jnp.exp(ref - cum)
    near_left = jnp.concatenate([unit * jnp.exp(exc - ref), recept * jnp.exp(cum - ref)], axis=0)
    near_right = jnp.concatenate([learned * down, key * down], axis=0)
    gone = jnp.full_like(cum, -1e30)
    far_down = jnp.exp(jnp.where(first, edge - cum, gone))
    far_left = jnp.concatenate(
        [
            unit * jnp.exp(jnp.where(first, gone, exc - edge)),
            recept * jnp.exp(jnp.where(first, gone, cum - edge)),
        ],
        axis=0,
    )
    far_right = jnp.concatenate([learned * far_down, key * far_down], axis=0)
    near = mm_nt(near_left, near_right)
    far = mm_nt(far_left, far_right)

    def part(up, left, mask):
        rows = slice(0, tokens) if up else slice(tokens, 2 * tokens)
        cols = slice(0, tokens) if left else slice(tokens, 2 * tokens)
        return jnp.where(mask, jnp.where(same, near[rows, cols], far[rows, cols]), 0.0)

    lower = part(True, True, before)
    unit_key = part(True, False, before)
    read_rank = part(False, True, upto)
    read_key = part(False, False, upto)
    eye = (i == j).astype(F32)
    inverse = eye - jnp.where((i // 2) == (j // 2), lower, 0.0)
    size = 2
    while size < half:
        link = jnp.where(((i // (2 * size)) == (j // (2 * size))) & ((i // size) != (j // size)), lower, 0.0)
        inverse = inverse - mm(inverse, mm(link, inverse))
        size *= 2
    written = mm(jnp.concatenate([unit_key, read_key], axis=0), value)
    right = jnp.concatenate([unit * jnp.exp(exc), written[:tokens]], axis=1)
    solved = mm(inverse, right)
    cross = jnp.where(same, 0.0, lower)
    solved = solved - mm(inverse, mm(cross, solved))
    reads = jnp.concatenate([recept * jnp.exp(cum), written[tokens:]], axis=1) - mm(read_rank, solved)
    tail = jnp.exp(total - cum)
    ki = lax.broadcasted_iota(jnp.int32, (width, width), 0)
    kj = lax.broadcasted_iota(jnp.int32, (width, width), 1)
    diag = jnp.where(ki == kj, jnp.broadcast_to(jnp.exp(total), (width, width)), 0.0)
    maps = jnp.concatenate([diag, mm_tn(key * tail, value)], axis=1) - mm_tn(learned * tail, solved)
    return reads, maps


def mixer_values(rows, gain, w_recept, w_key, w_value, w_low, decay_up, rate_up, decay_base, rate_base, shift):
    normed = norm_rows(rows, gain)

    def project(weight):
        return mm_nt(normed, weight, None).astype(BF16).astype(F32)

    recept, key, value = (project(w_recept), project(w_key), project(w_value))
    low = jnp.tanh(mm_nt(normed, w_low, None)).astype(BF16)
    tokens = rows.shape[0]
    i = lax.broadcasted_iota(jnp.int32, (tokens, tokens), 0)
    j = lax.broadcasted_iota(jnp.int32, (tokens, tokens), 1)
    shift = jnp.sum(jnp.where(i == j, shift, 0.0), axis=1, keepdims=True)
    log_decay = -DECAY_SCALE * jax.nn.sigmoid(decay_base + mm(low, decay_up, None)) + shift
    rate = jax.nn.sigmoid(rate_base + mm(low, rate_up, None))
    unit = key * lax.rsqrt(jnp.sum(key * key, axis=-1, keepdims=True) + 1e-06)
    ahead = block_totals(log_decay, unit, rate, key, value, recept, False)
    back = block_totals(log_decay, unit, rate, key, value, recept, True)
    return ahead, back


def mixer_kernel(*refs):
    ins, (reads_f, reads_b, maps) = refs[:11], refs[11:]
    ahead, back = mixer_values(*[ref[...] for ref in ins])
    reads_f[...] = ahead[0]
    reads_b[...] = back[0]
    width = ahead[1].shape[0]
    maps[:width] = ahead[1].astype(BF16)
    maps[width:] = back[1].astype(BF16)


def with_identity(maps):
    width = maps.shape[0]
    r = lax.broadcasted_iota(jnp.int32, maps.shape, 0)
    c = lax.broadcasted_iota(jnp.int32, maps.shape, 1)
    return jnp.concatenate([maps, (c == r + width).astype(maps.dtype)], axis=0)


def chained(blocks, reverse):
    level = blocks
    while len(level) > 1:
        last = len(level) == 2
        joined = []
        for k in range(0, len(level), 2):
            early, late = (level[k + 1], level[k]) if reverse else (level[k], level[k + 1])
            product = mm(late, with_identity(early), None)
            joined.append(product if last else product.astype(BF16))
        level = joined
    return level[0]


def plain_like(maps):
    r = lax.broadcasted_iota(jnp.int32, maps.shape, 0)
    c = lax.broadcasted_iota(jnp.int32, maps.shape, 1)
    return (r == c).astype(F32)


def kept(maps, use, plain):
    return jnp.where(use, maps.astype(F32), plain).astype(BF16)


def row_values(place, gathered):
    count = len(gathered)
    plain = plain_like(gathered[0][0])
    ahead, back = ([g[0] for g in gathered], [g[1] for g in gathered])
    before = chained([kept(ahead[k], k < place, plain) for k in range(count)], False)
    after = chained([kept(back[k], k > place, plain) for k in range(count)], True)
    return chained(ahead, False), chained(back, True), before, after


def row_kernel(place, high, *refs):
    held, (sent, before, after) = refs[:-3], refs[-3:]
    width = before.shape[0]
    count = len(held)
    held = [(r[:width], r[width:]) for r in held]
    at = place[0]
    gathered = []
    for k in range(count):
        far = lax.rem(at - k + count, count)
        chosen = []
        for side in range(2):
            value = held[0][side].astype(F32)
            for m in range(1, count):
                value = jnp.where(far == m, held[m][side].astype(F32), value)
            chosen.append(value.astype(BF16))
        gathered.append(chosen)
    total_f, total_b, before[...], after[...] = row_values(at, gathered)
    for k in range(sent.shape[0]):
        sent[k] = jnp.where(k > high[0], total_f, total_b).astype(BF16)


def output_values(place, core, arrived, before, after, reads_f, reads_b, gain, w_output, chips):
    count, width = len(arrived), before.shape[0]
    plain = plain_like(arrived[0])
    ahead = chained([kept(arrived[k], k < place, plain) for k in range(count)], False)
    back = chained([kept(arrived[k], k > place, plain) for k in range(count)], True)
    ahead = mm(before, with_identity(ahead))
    back = mm(after, with_identity(back))
    mixed = mm(reads_f, with_identity(ahead)) + mm(reads_b, with_identity(back))
    mixed = mixed[:, width:]
    centre = mixed - jnp.mean(mixed, axis=-1, keepdims=True)
    scaled = centre * lax.rsqrt(jnp.mean(centre * centre, axis=-1, keepdims=True) + 1e-05)
    grouped = scaled * gain
    split = grouped.reshape(chips, 2, -1, width)
    results = []
    for use in (core == 0, core != 0):
        rows = jnp.where(use, split[:, 0], split[:, 1]).reshape(-1, width)
        results.append(mm(rows.astype(BF16), w_output, None).astype(BF16))
    return results


def output_kernel(place, core, arrived, before, after, reads_f, reads_b, gain, w_output, own, away):
    values = output_values(
        place[0],
        core[0],
        [arrived[k] for k in range(arrived.shape[0])],
        before[...],
        after[...],
        reads_f[...],
        reads_b[...],
        gain[...],
        w_output[...],
        own.shape[0],
    )
    for out, value in zip((own, away), values):
        out[...] = value.reshape(out.shape)


def down_block(hidden, down, parity, width, y):
    columns = pl.ds(pl.multiple_of((2 * y + parity) * width, width), width)
    return mm(hidden, down[:, columns], None).astype(BF16)


def expert_kernel(width, core, arrived, swapped, gate, up, down, hidden, away):
    half = arrived.shape[1]
    at = core[0]
    near = pl.ds(pl.multiple_of(at * half, half), half)
    far = pl.ds(pl.multiple_of((1 - at) * half, half), half)
    pairs = [(arrived[...], near), (swapped[...], far)]
    gated = sum(mm(value, gate[where, :], None) for value, where in pairs)
    raised = sum(mm(value, up[where, :], None) for value, where in pairs)
    inner = (gated / (1.0 + jnp.exp(-gated)) * raised).astype(BF16)
    hidden[...] = inner
    for y in range(half // width):
        away[:, y * width : (y + 1) * width] = down_block(inner, down, 1 - at, width, y)


def pair_kernel(width, core, hidden, landed, down, out):
    inner = hidden[...]
    for y in range(out.shape[1] // width):
        columns = slice(y * width, (y + 1) * width)
        part = down_block(inner, down, core[0], width, y).astype(F32)
        out[:, columns] = (part + landed[:, columns].astype(F32)).astype(BF16)


def combine_kernel(returned, weighing, own, landed, out):
    chips, each, width = own.shape[0], own.shape[1], out.shape[2]
    tokens = weighing.shape[1]
    weighed = mm_tn(weighing[...], returned[...], None).astype(BF16)
    for y in range(chips):
        out[y, :tokens] = weighed[:, y * width : (y + 1) * width]
        joined = own[y].astype(F32) + landed[y].astype(F32)
        for k in range(own.shape[2] // width):
            rows = slice(tokens + k * each, tokens + (k + 1) * each)
            out[y, rows] = joined[:, k * width : (k + 1) * width].astype(BF16)


def finish_kernel(shares, mixed, moe):
    chips, width = shares.shape[0], shares.shape[2]
    tokens, each = moe.shape[0], mixed.shape[0]
    total = shares[0].astype(F32)
    for y in range(1, chips):
        total = total + shares[y].astype(F32)
    moe[...] = total[:tokens].astype(BF16)
    for k in range(mixed.shape[1] // width):
        rows = slice(tokens + k * each, tokens + (k + 1) * each)
        mixed[:, k * width : (k + 1) * width] = total[rows].astype(BF16)


def route_values(routes, weights, experts, slots):
    tokens = routes.shape[1]
    i = lax.broadcasted_iota(jnp.int32, (tokens, tokens), 0)
    j = lax.broadcasted_iota(jnp.int32, (tokens, tokens), 1)
    across = routes.astype(F32)
    along = weights.astype(BF16).astype(F32)
    expert = lax.broadcasted_iota(jnp.int32, (experts, tokens), 0).astype(F32)
    named = [(expert == across[k : k + 1]).astype(F32) for k in range(2)]
    earlier = mm((named[0] + named[1]).astype(BF16), (i < j).astype(BF16), None)
    row = lax.broadcasted_iota(jnp.int32, (experts * slots, tokens), 0).astype(F32)
    placing = jnp.zeros(row.shape, F32)
    weighing = jnp.zeros(row.shape, F32)
    for k in range(2):
        slot = jnp.sum(named[k] * earlier, axis=0, keepdims=True)
        match = row == across[k : k + 1] * slots + slot
        placing = placing + jnp.where(match, 1.0, 0.0)
        weighing = weighing + jnp.where(match, along[k : k + 1], 0.0)
    return placing.astype(BF16), weighing.astype(BF16)


def dispatch_kernel(experts, slots, core, rows, gain, routes, weights, buffer, weighing):
    placing, weigh = route_values(routes[...], weights[...], experts, slots)
    weighing[...] = weigh
    normed = norm_rows(rows[...], gain[...])
    width = normed.shape[1] // 2
    mine = jnp.where(core[0] == 0, normed[:, :width].astype(F32), normed[:, width:].astype(F32))
    buffer[...] = mm(placing, mine.astype(BF16), None).astype(BF16)


def call(kernel, outs, scalars, *args):
    smem = pl.BlockSpec(memory_space=pltpu.SMEM)
    vmem = pl.BlockSpec(memory_space=pltpu.VMEM)
    return pl.pallas_call(
        kernel,
        out_shape=outs,
        in_specs=[smem] * len(scalars) + [vmem] * len(args),
        out_specs=jax.tree.map(lambda _: vmem, outs),
    )(*scalars, *args)


def shards(
    mixer_input_rows,
    mix_gain,
    w_recept,
    w_key,
    w_value,
    lowered_map_factor,
    decay_up,
    rate_up,
    decay_base,
    rate_base,
    decay_shift,
    out_gain,
    w_output,
    moe_rows,
    moe_gain,
    routes,
    route_weight,
    exp_gate,
    exp_up,
    exp_down,
):
    experts, tp = (lax.axis_size("ep"), lax.axis_size("tp"))
    place, lane = (lax.axis_index("ep"), lax.axis_index("tp"))
    core = lane & 1
    chips = tp // 2
    across = ROW
    rows = experts // across
    high, low = (place // across, place % across)
    swap = [(k, k ^ 1) for k in range(tp)]
    tokens, model = moe_rows.shape
    slots = 4 * tokens // experts
    half = model // 2
    width = w_key.shape[1]
    piece = model // tp
    scalar = lambda v: v.astype(jnp.int32).reshape(1)
    shape = jax.ShapeDtypeStruct

    buffer, weighing = call(
        functools.partial(dispatch_kernel, experts, slots),
        (shape((experts * slots, half), BF16), shape((experts * slots, tokens), BF16)),
        (scalar(core),),
        moe_rows,
        moe_gain.reshape(1, -1),
        routes.T,
        route_weight.T,
    )
    arrived = lax.all_to_all(
        buffer.reshape(experts, slots, half), "ep", split_axis=0, concat_axis=0, tiled=True
    ).reshape(experts * slots, half)

    reads = shape((tokens, 2 * width), F32)
    wide = shape((width, 2 * width), F32)
    reads_f, reads_b, both = call(
        mixer_kernel,
        (reads, reads, shape((2 * width, 2 * width), BF16)),
        (),
        mixer_input_rows,
        mix_gain.reshape(1, -1),
        w_recept.T,
        w_key.T,
        w_value.T,
        lowered_map_factor.T,
        decay_up,
        rate_up,
        decay_base.reshape(1, -1),
        rate_base.reshape(1, -1),
        decay_shift.T,
    )

    others = [
        lax.ppermute(
            both,
            "ep",
            [(k, k // across * across + (k + m) % across) for k in range(experts)],
        )
        for m in range(1, across)
    ]
    sent, before, after = call(
        row_kernel,
        (shape((rows, width, 2 * width), BF16), wide, wide),
        (scalar(low), scalar(high)),
        both,
        *others,
    )

    arrived, sent = lax.optimization_barrier((arrived, sent))

    carried = lax.all_to_all(
        sent,
        "ep",
        split_axis=0,
        concat_axis=0,
        tiled=True,
        axis_index_groups=[[z * across + x for z in range(rows)] for x in range(across)],
    )

    swapped = lax.ppermute(arrived, "tp", swap)
    inner = exp_gate.shape[2]
    hidden, away = call(
        functools.partial(expert_kernel, piece),
        (shape((experts * slots, inner), BF16), shape((experts * slots, half), BF16)),
        (scalar(core),),
        arrived,
        swapped,
        exp_gate[0],
        exp_up[0],
        exp_down[0],
    )
    landed = lax.ppermute(away, "tp", swap)
    paired = call(
        functools.partial(pair_kernel, piece),
        shape((experts * slots, half), BF16),
        (scalar(core),),
        hidden,
        landed,
        exp_down[0],
    )

    returned = lax.all_to_all(
        paired.reshape(experts, slots, half), "ep", split_axis=0, concat_axis=0, tiled=True
    ).reshape(experts * slots, half)

    shares = shape((chips, tokens // tp, model), BF16)
    own_rows, away_rows = call(
        output_kernel,
        (shares, shares),
        (scalar(high), scalar(core)),
        carried,
        before,
        after,
        reads_f,
        reads_b,
        out_gain.reshape(1, -1),
        w_output,
    )
    landed_rows = lax.ppermute(away_rows, "tp", swap)

    parts = call(
        combine_kernel,
        shape((chips, 2 * tokens, piece), BF16),
        (),
        returned,
        weighing,
        own_rows,
        landed_rows,
    )
    parts = lax.all_to_all(
        parts,
        "tp",
        split_axis=0,
        concat_axis=0,
        tiled=True,
        axis_index_groups=[[2 * y + c for y in range(chips)] for c in range(2)],
    )
    mix_out, moe_out = call(
        finish_kernel,
        (shape((tokens // tp, model), BF16), shape((tokens, piece), BF16)),
        (),
        parts,
    )
    return (mix_out, moe_out)


def solution(mesh):
    return jax.shard_map(
        shards,
        mesh=mesh,
        in_specs=(
            P("ep", None),
            P(),
            P(None, "tp"),
            P(None, "tp"),
            P(None, "tp"),
            P(),
            P(None, "tp"),
            P(None, "tp"),
            P("tp"),
            P("tp"),
            P("ep", "tp"),
            P("tp"),
            P("tp", None),
            P("ep", None),
            P(),
            P("ep", None),
            P("ep", None),
            P("ep", None, "tp"),
            P("ep", None, "tp"),
            P("ep", "tp", None),
        ),
        out_specs=(P(("ep", "tp"), None), P("ep", "tp")),
        check_vma=False,
    )
```

```python
import functools
import math

import jax
import jax.numpy as jnp
from jax import lax
from jax.experimental import pallas as pl
from jax.experimental.pallas import tpu as pltpu
from jax.sharding import PartitionSpec as P


DECAY_SCALE = math.exp(-0.5)
HIGH = lax.Precision.HIGHEST
F32 = jnp.float32
BF16 = jnp.bfloat16
ROW = 4
LIMIT = 24 * 1024 * 1024


def mm(a, b, precision=HIGH):
    return lax.dot_general(
        a, b, (((1,), (0,)), ((), ())), precision=precision, preferred_element_type=F32
    )


def mm_nt(a, b, precision=HIGH):
    return lax.dot_general(
        a, b, (((1,), (1,)), ((), ())), precision=precision, preferred_element_type=F32
    )


def mm_tn(a, b, precision=HIGH):
    return lax.dot_general(
        a, b, (((0,), (0,)), ((), ())), precision=precision, preferred_element_type=F32
    )


def norm_rows(rows, gain):
    entries = rows.astype(F32)
    factor = lax.rsqrt(jnp.mean(entries * entries, axis=-1, keepdims=True) + 1e-06)
    return (entries * factor * gain).astype(BF16)


def block_totals(log_decay, unit, rate, key, value, recept, reverse):
    tokens, width = log_decay.shape
    half = tokens // 2
    i = lax.broadcasted_iota(jnp.int32, (tokens, tokens), 0)
    j = lax.broadcasted_iota(jnp.int32, (tokens, tokens), 1)
    upto = (j >= i) if reverse else (j <= i)
    before = (j > i) if reverse else (j < i)
    same = (i // half) == (j // half)
    cum = mm(upto.astype(F32), log_decay)
    exc = cum - log_decay
    row = lax.broadcasted_iota(jnp.int32, (tokens, width), 0)
    if reverse:
        total = cum[:1]
        edge = cum[half : half + 1]
        first = row >= half
        mid_low, mid_high = (half // 2, half + half // 2)
    else:
        total = cum[tokens - 1 :]
        edge = cum[half - 1 : half]
        first = row < half
        mid_low, mid_high = (half // 2 - 1, half + half // 2 - 1)
    ref = jnp.where(row < half, cum[mid_low : mid_low + 1], cum[mid_high : mid_high + 1])
    learned = unit * rate
    down = jnp.exp(ref - cum)
    near_left = jnp.concatenate([unit * jnp.exp(exc - ref), recept * jnp.exp(cum - ref)], axis=0)
    near_right = jnp.concatenate([learned * down, key * down], axis=0)
    gone = jnp.full_like(cum, -1e30)
    far_down = jnp.exp(jnp.where(first, edge - cum, gone))
    far_left = jnp.concatenate(
        [
            unit * jnp.exp(jnp.where(first, gone, exc - edge)),
            recept * jnp.exp(jnp.where(first, gone, cum - edge)),
        ],
        axis=0,
    )
    far_right = jnp.concatenate([learned * far_down, key * far_down], axis=0)
    near = mm_nt(near_left, near_right)
    far = mm_nt(far_left, far_right)

    def part(up, left, mask):
        rows = slice(0, tokens) if up else slice(tokens, 2 * tokens)
        cols = slice(0, tokens) if left else slice(tokens, 2 * tokens)
        return jnp.where(mask, jnp.where(same, near[rows, cols], far[rows, cols]), 0.0)

    lower = part(True, True, before)
    unit_key = part(True, False, before)
    read_rank = part(False, True, upto)
    read_key = part(False, False, upto)
    eye = (i == j).astype(F32)
    inverse = eye - jnp.where((i // 2) == (j // 2), lower, 0.0)
    size = 2
    while size < half:
        link = jnp.where(((i // (2 * size)) == (j // (2 * size))) & ((i // size) != (j // size)), lower, 0.0)
        inverse = inverse - mm(inverse, mm(link, inverse))
        size *= 2
    written = mm(jnp.concatenate([unit_key, read_key], axis=0), value)
    right = jnp.concatenate([unit * jnp.exp(exc), written[:tokens]], axis=1)
    solved = mm(inverse, right)
    cross = jnp.where(same, 0.0, lower)
    solved = solved - mm(inverse, mm(cross, solved))
    reads = jnp.concatenate([recept * jnp.exp(cum), written[tokens:]], axis=1) - mm(read_rank, solved)
    tail = jnp.exp(total - cum)
    ki = lax.broadcasted_iota(jnp.int32, (width, width), 0)
    kj = lax.broadcasted_iota(jnp.int32, (width, width), 1)
    diag = jnp.where(ki == kj, jnp.broadcast_to(jnp.exp(total), (width, width)), 0.0)
    maps = jnp.concatenate([diag, mm_tn(key * tail, value)], axis=1) - mm_tn(learned * tail, solved)
    return reads, maps


def mixer_values(rows, gain, w_recept, w_key, w_value, w_low, decay_up, rate_up, decay_base, rate_base, shift):
    normed = norm_rows(rows, gain)

    def project(weight):
        return mm_nt(normed, weight, None).astype(BF16).astype(F32)

    recept, key, value = (project(w_recept), project(w_key), project(w_value))
    low = jnp.tanh(mm_nt(normed, w_low, None)).astype(BF16)
    tokens = rows.shape[0]
    i = lax.broadcasted_iota(jnp.int32, (tokens, tokens), 0)
    j = lax.broadcasted_iota(jnp.int32, (tokens, tokens), 1)
    shift = jnp.sum(jnp.where(i == j, shift, 0.0), axis=1, keepdims=True)
    log_decay = -DECAY_SCALE * jax.nn.sigmoid(decay_base + mm(low, decay_up, None)) + shift
    rate = jax.nn.sigmoid(rate_base + mm(low, rate_up, None))
    unit = key * lax.rsqrt(jnp.sum(key * key, axis=-1, keepdims=True) + 1e-06)
    ahead = block_totals(log_decay, unit, rate, key, value, recept, False)
    back = block_totals(log_decay, unit, rate, key, value, recept, True)
    return ahead, back


def mixer_kernel(*refs):
    ins, (reads_f, reads_b, maps) = refs[:11], refs[11:]
    ahead, back = mixer_values(*[ref[...] for ref in ins])
    reads_f[...] = ahead[0]
    reads_b[...] = back[0]
    width = ahead[1].shape[0]
    maps[:width] = ahead[1].astype(BF16)
    maps[width:] = back[1].astype(BF16)


def with_identity(maps):
    width = maps.shape[0]
    r = lax.broadcasted_iota(jnp.int32, maps.shape, 0)
    c = lax.broadcasted_iota(jnp.int32, maps.shape, 1)
    return jnp.concatenate([maps, (c == r + width).astype(maps.dtype)], axis=0)


def chained(blocks, reverse):
    level = blocks
    while len(level) > 1:
        last = len(level) == 2
        joined = []
        for k in range(0, len(level), 2):
            early, late = (level[k + 1], level[k]) if reverse else (level[k], level[k + 1])
            product = mm(late, with_identity(early), None)
            joined.append(product if last else product.astype(BF16))
        level = joined
    return level[0]


def plain_like(maps):
    r = lax.broadcasted_iota(jnp.int32, maps.shape, 0)
    c = lax.broadcasted_iota(jnp.int32, maps.shape, 1)
    return (r == c).astype(F32)


def kept(maps, use, plain):
    return jnp.where(use, maps.astype(F32), plain).astype(BF16)


def row_values(place, gathered):
    count = len(gathered)
    plain = plain_like(gathered[0][0])
    ahead, back = ([g[0] for g in gathered], [g[1] for g in gathered])
    before = chained([kept(ahead[k], k < place, plain) for k in range(count)], False)
    after = chained([kept(back[k], k > place, plain) for k in range(count)], True)
    return chained(ahead, False), chained(back, True), before, after


def row_kernel(place, high, *refs):
    held, (sent, before, after) = refs[:-3], refs[-3:]
    width = before.shape[0]
    count = len(held)
    held = [(r[:width], r[width:]) for r in held]
    at = place[0]
    gathered = []
    for k in range(count):
        far = lax.rem(at - k + count, count)
        chosen = []
        for side in range(2):
            value = held[0][side].astype(F32)
            for m in range(1, count):
                value = jnp.where(far == m, held[m][side].astype(F32), value)
            chosen.append(value.astype(BF16))
        gathered.append(chosen)
    total_f, total_b, before[...], after[...] = row_values(at, gathered)
    for k in range(sent.shape[0]):
        sent[k] = jnp.where(k > high[0], total_f, total_b).astype(BF16)


def output_values(place, core, arrived, before, after, reads_f, reads_b, gain, w_output, chips):
    count, width = len(arrived), before.shape[0]
    plain = plain_like(arrived[0])
    ahead = chained([kept(arrived[k], k < place, plain) for k in range(count)], False)
    back = chained([kept(arrived[k], k > place, plain) for k in range(count)], True)
    ahead = mm(before, with_identity(ahead))
    back = mm(after, with_identity(back))
    mixed = mm(reads_f, with_identity(ahead)) + mm(reads_b, with_identity(back))
    mixed = mixed[:, width:]
    centre = mixed - jnp.mean(mixed, axis=-1, keepdims=True)
    scaled = centre * lax.rsqrt(jnp.mean(centre * centre, axis=-1, keepdims=True) + 1e-05)
    grouped = scaled * gain
    split = grouped.reshape(chips, 2, -1, width)
    results = []
    for use in (core == 0, core != 0):
        rows = jnp.where(use, split[:, 0], split[:, 1]).reshape(-1, width)
        results.append(mm(rows.astype(BF16), w_output, None).astype(BF16))
    return results


def output_kernel(place, core, arrived, before, after, reads_f, reads_b, gain, w_output, own, away):
    values = output_values(
        place[0],
        core[0],
        [arrived[k] for k in range(arrived.shape[0])],
        before[...],
        after[...],
        reads_f[...],
        reads_b[...],
        gain[...],
        w_output[...],
        own.shape[0],
    )
    for out, value in zip((own, away), values):
        out[...] = value.reshape(out.shape)


def down_block(hidden, down, parity, width, y):
    columns = pl.ds(pl.multiple_of((2 * y + parity) * width, width), width)
    return mm(hidden, down[:, columns], None).astype(BF16)


def expert_kernel(width, core, arrived, swapped, gate, up, down, hidden, away):
    half = arrived.shape[1]
    at = core[0]
    near = pl.ds(pl.multiple_of(at * half, half), half)
    far = pl.ds(pl.multiple_of((1 - at) * half, half), half)
    pairs = [(arrived[...], near), (swapped[...], far)]
    gated = sum(mm(value, gate[where, :], None) for value, where in pairs)
    raised = sum(mm(value, up[where, :], None) for value, where in pairs)
    inner = (gated / (1.0 + jnp.exp(-gated)) * raised).astype(BF16)
    hidden[...] = inner
    for y in range(half // width):
        away[:, y * width : (y + 1) * width] = down_block(inner, down, 1 - at, width, y)


def pair_kernel(width, core, hidden, landed, down, out):
    inner = hidden[...]
    for y in range(out.shape[1] // width):
        columns = slice(y * width, (y + 1) * width)
        part = down_block(inner, down, core[0], width, y).astype(F32)
        out[:, columns] = (part + landed[:, columns].astype(F32)).astype(BF16)


def combine_kernel(returned, weighing, own, landed, out):
    chips, each, width = own.shape[0], own.shape[1], out.shape[2]
    tokens = weighing.shape[1]
    weighed = mm_tn(weighing[...], returned[...], None).astype(BF16)
    for y in range(chips):
        out[y, :tokens] = weighed[:, y * width : (y + 1) * width]
        joined = own[y].astype(F32) + landed[y].astype(F32)
        for k in range(own.shape[2] // width):
            rows = slice(tokens + k * each, tokens + (k + 1) * each)
            out[y, rows] = joined[:, k * width : (k + 1) * width].astype(BF16)


def finish_kernel(shares, mixed, moe):
    chips, width = shares.shape[0], shares.shape[2]
    tokens, each = moe.shape[0], mixed.shape[0]
    total = shares[0].astype(F32)
    for y in range(1, chips):
        total = total + shares[y].astype(F32)
    moe[...] = total[:tokens].astype(BF16)
    for k in range(mixed.shape[1] // width):
        rows = slice(tokens + k * each, tokens + (k + 1) * each)
        mixed[:, k * width : (k + 1) * width] = total[rows].astype(BF16)


def route_values(routes, weights, experts, slots):
    tokens = routes.shape[1]
    i = lax.broadcasted_iota(jnp.int32, (tokens, tokens), 0)
    j = lax.broadcasted_iota(jnp.int32, (tokens, tokens), 1)
    across = routes.astype(F32)
    along = weights.astype(BF16).astype(F32)
    expert = lax.broadcasted_iota(jnp.int32, (experts, tokens), 0).astype(F32)
    named = [(expert == across[k : k + 1]).astype(F32) for k in range(2)]
    earlier = mm((named[0] + named[1]).astype(BF16), (i < j).astype(BF16), None)
    row = lax.broadcasted_iota(jnp.int32, (experts * slots, tokens), 0).astype(F32)
    placing = jnp.zeros(row.shape, F32)
    weighing = jnp.zeros(row.shape, F32)
    for k in range(2):
        slot = jnp.sum(named[k] * earlier, axis=0, keepdims=True)
        match = row == across[k : k + 1] * slots + slot
        placing = placing + jnp.where(match, 1.0, 0.0)
        weighing = weighing + jnp.where(match, along[k : k + 1], 0.0)
    return placing.astype(BF16), weighing.astype(BF16)


def dispatch_kernel(experts, slots, core, rows, gain, routes, weights, buffer, weighing):
    placing, weigh = route_values(routes[...], weights[...], experts, slots)
    weighing[...] = weigh
    normed = norm_rows(rows[...], gain[...])
    width = normed.shape[1] // 2
    mine = jnp.where(core[0] == 0, normed[:, :width].astype(F32), normed[:, width:].astype(F32))
    buffer[...] = mm(placing, mine.astype(BF16), None).astype(BF16)


def placed(value, space):
    if isinstance(value, jax.ShapeDtypeStruct):
        return space(value.shape, value.dtype)
    return pltpu.with_memory_space_constraint(value, space)


near = lambda value: placed(value, pltpu.VMEM)
far = lambda value: placed(value, pltpu.HBM)


def call(kernel, outs, scalars, *args):
    smem = pl.BlockSpec(memory_space=pltpu.SMEM)
    vmem = pl.BlockSpec(memory_space=pltpu.VMEM)
    return pl.pallas_call(
        kernel,
        out_shape=outs,
        in_specs=[smem] * len(scalars) + [vmem] * len(args),
        out_specs=jax.tree.map(lambda _: vmem, outs),
        compiler_params=pltpu.CompilerParams(vmem_limit_bytes=LIMIT),
    )(*scalars, *args)


def shards(
    mixer_input_rows,
    mix_gain,
    w_recept,
    w_key,
    w_value,
    lowered_map_factor,
    decay_up,
    rate_up,
    decay_base,
    rate_base,
    decay_shift,
    out_gain,
    w_output,
    moe_rows,
    moe_gain,
    routes,
    route_weight,
    exp_gate,
    exp_up,
    exp_down,
):
    experts, tp = (lax.axis_size("ep"), lax.axis_size("tp"))
    place, lane = (lax.axis_index("ep"), lax.axis_index("tp"))
    core = lane & 1
    chips = tp // 2
    across = ROW
    rows = experts // across
    high, low = (place // across, place % across)
    swap = [(k, k ^ 1) for k in range(tp)]
    tokens, model = moe_rows.shape
    slots = 4 * tokens // experts
    half = model // 2
    width = w_key.shape[1]
    piece = model // tp
    scalar = lambda v: v.astype(jnp.int32).reshape(1)
    shape = jax.ShapeDtypeStruct

    buffer, weighing = call(
        functools.partial(dispatch_kernel, experts, slots),
        (shape((experts * slots, half), BF16), far(shape((experts * slots, tokens), BF16))),
        (scalar(core),),
        far(moe_rows),
        far(moe_gain.reshape(1, -1)),
        far(routes.T),
        far(route_weight.T),
    )
    arrived = lax.all_to_all(
        buffer.reshape(experts, slots, half), "ep", split_axis=0, concat_axis=0, tiled=True
    ).reshape(experts * slots, half)

    reads = far(shape((tokens, 2 * width), F32))
    wide = far(shape((width, 2 * width), F32))
    reads_f, reads_b, both = call(
        mixer_kernel,
        (reads, reads, near(shape((2 * width, 2 * width), BF16))),
        (),
        far(mixer_input_rows),
        far(mix_gain.reshape(1, -1)),
        far(w_recept.T),
        far(w_key.T),
        far(w_value.T),
        far(lowered_map_factor.T),
        far(decay_up),
        far(rate_up),
        far(decay_base.reshape(1, -1)),
        far(rate_base.reshape(1, -1)),
        far(decay_shift.T),
    )

    others = [
        lax.ppermute(
            both,
            "ep",
            [(k, k // across * across + (k + m) % across) for k in range(experts)],
        )
        for m in range(1, across)
    ]
    sent, before, after = call(
        row_kernel,
        (near(shape((rows, width, 2 * width), BF16)), wide, wide),
        (scalar(low), scalar(high)),
        near(both),
        *[near(other) for other in others],
    )

    arrived, sent = lax.optimization_barrier((arrived, sent))

    carried = lax.all_to_all(
        sent,
        "ep",
        split_axis=0,
        concat_axis=0,
        tiled=True,
        axis_index_groups=[[z * across + x for z in range(rows)] for x in range(across)],
    )

    swapped = lax.ppermute(arrived, "tp", swap)
    inner = exp_gate.shape[2]
    hidden, away = call(
        functools.partial(expert_kernel, piece),
        (near(shape((experts * slots, inner), BF16)), near(shape((experts * slots, half), BF16))),
        (scalar(core),),
        near(arrived),
        near(swapped),
        far(exp_gate[0]),
        near(exp_up[0]),
        near(exp_down[0]),
    )
    landed = lax.ppermute(away, "tp", swap)
    paired = call(
        functools.partial(pair_kernel, piece),
        near(shape((experts * slots, half), BF16)),
        (scalar(core),),
        near(hidden),
        near(landed),
        near(exp_down[0]),
    )

    returned = lax.all_to_all(
        paired.reshape(experts, slots, half), "ep", split_axis=0, concat_axis=0, tiled=True
    ).reshape(experts * slots, half)

    shares = shape((chips, tokens // tp, model), BF16)
    own_rows, away_rows = call(
        output_kernel,
        (near(shares), near(shares)),
        (scalar(high), scalar(core)),
        near(carried),
        far(before),
        far(after),
        far(reads_f),
        far(reads_b),
        far(out_gain.reshape(1, -1)),
        far(w_output),
    )
    landed_rows = lax.ppermute(away_rows, "tp", swap)

    parts = call(
        combine_kernel,
        near(shape((chips, 2 * tokens, piece), BF16)),
        (),
        near(returned),
        far(weighing),
        near(own_rows),
        near(landed_rows),
    )
    parts = lax.all_to_all(
        parts,
        "tp",
        split_axis=0,
        concat_axis=0,
        tiled=True,
        axis_index_groups=[[2 * y + c for y in range(chips)] for c in range(2)],
    )
    mix_out, moe_out = call(
        finish_kernel,
        (shape((tokens // tp, model), BF16), shape((tokens, piece), BF16)),
        (),
        near(parts),
    )
    return (mix_out, moe_out)


def solution(mesh):
    return jax.shard_map(
        shards,
        mesh=mesh,
        in_specs=(
            P("ep", None),
            P(),
            P(None, "tp"),
            P(None, "tp"),
            P(None, "tp"),
            P(),
            P(None, "tp"),
            P(None, "tp"),
            P("tp"),
            P("tp"),
            P("ep", "tp"),
            P("tp"),
            P("tp", None),
            P("ep", None),
            P(),
            P("ep", None),
            P("ep", None),
            P("ep", None, "tp"),
            P("ep", None, "tp"),
            P("ep", "tp", None),
        ),
        out_specs=(P(("ep", "tp"), None), P("ep", "tp")),
        check_vma=False,
    )
```

```python
import functools
import math

import jax
import jax.numpy as jnp
from jax import lax
from jax.experimental import pallas as pl
from jax.experimental.pallas import tpu as pltpu
from jax.sharding import PartitionSpec as P


DECAY_SCALE = math.exp(-0.5)
HIGH = lax.Precision.HIGH
F32 = jnp.float32
BF16 = jnp.bfloat16
BLOCK = 256
LIMIT = 16 * 1024 * 1024


def mm(a, b, precision=HIGH):
    return lax.dot_general(
        a, b, (((1,), (0,)), ((), ())), precision=precision, preferred_element_type=F32
    )


def mm_nt(a, b, precision=HIGH):
    return lax.dot_general(
        a, b, (((1,), (1,)), ((), ())), precision=precision, preferred_element_type=F32
    )


def mm_tn(a, b, precision=HIGH):
    return lax.dot_general(
        a, b, (((0,), (0,)), ((), ())), precision=precision, preferred_element_type=F32
    )


def norm_rows(rows, gain):
    entries = rows.astype(F32)
    factor = lax.rsqrt(jnp.mean(entries * entries, axis=-1, keepdims=True) + 1e-06)
    return (entries * factor * gain).astype(BF16)


def block_totals(log_decay, unit, rate, key, value, recept, reverse):
    tokens, width = log_decay.shape
    half = tokens // 2
    i = lax.broadcasted_iota(jnp.int32, (tokens, tokens), 0)
    j = lax.broadcasted_iota(jnp.int32, (tokens, tokens), 1)
    upto = (j >= i) if reverse else (j <= i)
    before = (j > i) if reverse else (j < i)
    same = (i // half) == (j // half)
    cum = mm(upto.astype(F32), log_decay)
    exc = cum - log_decay
    row = lax.broadcasted_iota(jnp.int32, (tokens, width), 0)
    if reverse:
        total = cum[:1]
        edge = cum[half : half + 1]
        first = row >= half
        mid_low, mid_high = (half // 2, half + half // 2)
    else:
        total = cum[tokens - 1 :]
        edge = cum[half - 1 : half]
        first = row < half
        mid_low, mid_high = (half // 2 - 1, half + half // 2 - 1)
    ref = jnp.where(row < half, cum[mid_low : mid_low + 1], cum[mid_high : mid_high + 1])
    learned = unit * rate
    down = jnp.exp(ref - cum)
    near_left = jnp.concatenate([unit * jnp.exp(exc - ref), recept * jnp.exp(cum - ref)], axis=0)
    near_right = jnp.concatenate([learned * down, key * down], axis=0)
    gone = jnp.full_like(cum, -1e30)
    far_down = jnp.exp(jnp.where(first, edge - cum, gone))
    far_left = jnp.concatenate(
        [
            unit * jnp.exp(jnp.where(first, gone, exc - edge)),
            recept * jnp.exp(jnp.where(first, gone, cum - edge)),
        ],
        axis=0,
    )
    far_right = jnp.concatenate([learned * far_down, key * far_down], axis=0)
    near = mm_nt(near_left, near_right)
    far = mm_nt(far_left, far_right)

    def part(up, left, mask):
        rows = slice(0, tokens) if up else slice(tokens, 2 * tokens)
        cols = slice(0, tokens) if left else slice(tokens, 2 * tokens)
        return jnp.where(mask, jnp.where(same, near[rows, cols], far[rows, cols]), 0.0)

    lower = part(True, True, before)
    unit_key = part(True, False, before)
    read_rank = part(False, True, upto)
    read_key = part(False, False, upto)
    eye = (i == j).astype(F32)
    inverse = eye - jnp.where((i // 2) == (j // 2), lower, 0.0)
    size = 2
    while size < half:
        link = jnp.where(((i // (2 * size)) == (j // (2 * size))) & ((i // size) != (j // size)), lower, 0.0)
        inverse = inverse - mm(inverse, mm(link, inverse))
        size *= 2
    written = mm(jnp.concatenate([unit_key, read_key], axis=0), value)
    right = jnp.concatenate([unit * jnp.exp(exc), written[:tokens]], axis=1)
    solved = mm(inverse, right)
    cross = jnp.where(same, 0.0, lower)
    solved = solved - mm(inverse, mm(cross, solved))
    reads = jnp.concatenate([recept * jnp.exp(cum), written[tokens:]], axis=1) - mm(read_rank, solved)
    tail = jnp.exp(total - cum)
    ki = lax.broadcasted_iota(jnp.int32, (width, width), 0)
    kj = lax.broadcasted_iota(jnp.int32, (width, width), 1)
    diag = jnp.where(ki == kj, jnp.broadcast_to(jnp.exp(total), (width, width)), 0.0)
    maps = jnp.concatenate([diag, mm_tn(key * tail, value)], axis=1) - mm_tn(learned * tail, solved)
    return reads, maps


def mixer_values(rows, gain, w_recept, w_key, w_value, w_low, decay_up, rate_up, decay_base, rate_base, shift):
    normed = norm_rows(rows, gain)

    def project(weight):
        return mm_nt(normed, weight, None).astype(BF16).astype(F32)

    recept, key, value = (project(w_recept), project(w_key), project(w_value))
    low = jnp.tanh(mm_nt(normed, w_low, None)).astype(BF16)
    tokens = rows.shape[0]
    i = lax.broadcasted_iota(jnp.int32, (tokens, tokens), 0)
    j = lax.broadcasted_iota(jnp.int32, (tokens, tokens), 1)
    shift = jnp.sum(jnp.where(i == j, shift, 0.0), axis=1, keepdims=True)
    log_decay = -DECAY_SCALE * jax.nn.sigmoid(decay_base + mm(low, decay_up, None)) + shift
    rate = jax.nn.sigmoid(rate_base + mm(low, rate_up, None))
    unit = key * lax.rsqrt(jnp.sum(key * key, axis=-1, keepdims=True) + 1e-06)
    ahead = block_totals(log_decay, unit, rate, key, value, recept, False)
    back = block_totals(log_decay, unit, rate, key, value, recept, True)
    return ahead, back


def mixer_kernel(*refs):
    ins, (reads_f, reads_b, maps) = refs[:11], refs[11:]
    ahead, back = mixer_values(*[ref[...] for ref in ins])
    reads_f[...] = ahead[0]
    reads_b[...] = back[0]
    width = ahead[1].shape[0]
    maps[:width] = ahead[1].astype(BF16)
    maps[width:] = back[1].astype(BF16)


def with_identity(maps):
    width = maps.shape[0]
    r = lax.broadcasted_iota(jnp.int32, maps.shape, 0)
    c = lax.broadcasted_iota(jnp.int32, maps.shape, 1)
    return jnp.concatenate([maps, (c == r + width).astype(maps.dtype)], axis=0)


def chained(blocks, reverse):
    level = blocks
    while len(level) > 1:
        last = len(level) == 2
        joined = []
        for k in range(0, len(level), 2):
            early, late = (level[k + 1], level[k]) if reverse else (level[k], level[k + 1])
            product = mm(late, with_identity(early), None)
            joined.append(product if last else product.astype(BF16))
        level = joined
    return level[0]


def plain_like(maps):
    r = lax.broadcasted_iota(jnp.int32, maps.shape, 0)
    c = lax.broadcasted_iota(jnp.int32, maps.shape, 1)
    return (r == c).astype(F32)


def kept(maps, use, plain):
    return jnp.where(use, maps.astype(F32), plain).astype(BF16)


def composed(late, early):
    return mm(late.astype(BF16), with_identity(early.astype(BF16)), None)


def joined(high, mine, theirs, before, after):
    width = before.shape[0]
    r = lax.broadcasted_iota(jnp.int32, before.shape, 0)
    c = lax.broadcasted_iota(jnp.int32, before.shape, 1)
    plain = (r == c).astype(F32)
    mine_f, mine_b = (mine[:width].astype(F32), mine[width:].astype(F32))
    their_f, their_b = (theirs[:width].astype(F32), theirs[width:].astype(F32))
    before = composed(before, jnp.where(high, their_f, plain))
    after = composed(after, jnp.where(high, plain, their_b))
    ahead = composed(jnp.where(high, mine_f, their_f), jnp.where(high, their_f, mine_f))
    back = composed(jnp.where(high, their_b, mine_b), jnp.where(high, mine_b, their_b))
    return ahead, back, before, after


def first_kernel(high, mine, theirs, total, before, after):
    width = before.shape[0]
    r = lax.broadcasted_iota(jnp.int32, before.shape, 0)
    c = lax.broadcasted_iota(jnp.int32, before.shape, 1)
    plain = (r == c).astype(F32)
    ahead, back, before[...], after[...] = joined(high[0] != 0, mine[...], theirs[...], plain, plain)
    total[:width] = ahead.astype(BF16)
    total[width:] = back.astype(BF16)


def send_kernel(high, run, mine, theirs, before_in, after_in, sent, before, after):
    ahead, back, before[...], after[...] = joined(
        high[0] != 0, mine[...], theirs[...], before_in[...], after_in[...]
    )
    for k in range(sent.shape[0]):
        sent[k] = jnp.where(k > run[0], ahead, back).astype(BF16)


def output_kernel(
    run, core, arrived, before, after, reads_f, reads_b, gain, w_output, own, away
):
    count, width = arrived.shape[0], before.shape[0]
    plain = plain_like(arrived[0])
    ahead = chained([kept(arrived[k], k < run[0], plain) for k in range(count)], False)
    back = chained([kept(arrived[k], k > run[0], plain) for k in range(count)], True)
    ahead = mm(before[...], with_identity(ahead))
    back = mm(after[...], with_identity(back))
    mixed = mm(reads_f[...], with_identity(ahead)) + mm(reads_b[...], with_identity(back))
    mixed = mixed[:, width:]
    centre = mixed - jnp.mean(mixed, axis=-1, keepdims=True)
    scaled = centre * lax.rsqrt(jnp.mean(centre * centre, axis=-1, keepdims=True) + 1e-05)
    split = (scaled * gain[...]).reshape(own.shape[0], 2, -1, width)
    for out, use in ((own, core[0] == 0), (away, core[0] != 0)):
        rows = jnp.where(use, split[:, 0], split[:, 1]).reshape(-1, width)
        out[...] = mm(rows.astype(BF16), w_output[...], None).astype(BF16).reshape(out.shape)


def sort_kernel(width, core, gate, down, held, own, away):
    held[...] = gate[...]
    for out, parity in ((own, core[0]), (away, 1 - core[0])):
        for y in range(out.shape[1] // width):
            columns = pl.ds(pl.multiple_of((2 * y + parity) * width, width), width)
            out[:, y * width : (y + 1) * width] = down[:, columns]


def expert_kernel(core, arrived, swapped, gate, up, hidden):
    half = arrived.shape[1]
    at = core[0]
    near_rows = pl.ds(pl.multiple_of(at * half, half), half)
    far_rows = pl.ds(pl.multiple_of((1 - at) * half, half), half)
    pairs = [(arrived[...], near_rows), (swapped[...], far_rows)]
    gated = sum(mm(value, gate[where, :], None) for value, where in pairs)
    raised = sum(mm(value, up[where, :], None) for value, where in pairs)
    hidden[...] = (gated / (1.0 + jnp.exp(-gated)) * raised).astype(BF16)


def pair_kernel(hidden, landed, own, other, out):
    rows = jnp.concatenate([hidden[...], landed[...]], axis=1)
    for k in range(0, out.shape[1], BLOCK):
        columns = slice(k, k + BLOCK)
        weight = jnp.concatenate([own[:, columns], other[:, columns]], axis=0)
        out[:, columns] = mm(rows, weight, None).astype(BF16)


def combine_kernel(returned, weighing, own, landed, out):
    chips, each, width = own.shape[0], own.shape[1], out.shape[2]
    tokens = weighing.shape[1]
    weighed = mm_tn(weighing[...], returned[...], None).astype(BF16)
    for y in range(chips):
        out[y, :tokens] = weighed[:, y * width : (y + 1) * width]
        total = own[y].astype(F32) + landed[y].astype(F32)
        for k in range(own.shape[2] // width):
            rows = slice(tokens + k * each, tokens + (k + 1) * each)
            out[y, rows] = total[:, k * width : (k + 1) * width].astype(BF16)


def finish_kernel(shares, mixed, moe):
    chips, width = shares.shape[0], shares.shape[2]
    tokens, each = moe.shape[0], mixed.shape[0]
    total = shares[0].astype(F32)
    for y in range(1, chips):
        total = total + shares[y].astype(F32)
    moe[...] = total[:tokens].astype(BF16)
    for k in range(mixed.shape[1] // width):
        rows = slice(tokens + k * each, tokens + (k + 1) * each)
        mixed[:, k * width : (k + 1) * width] = total[rows].astype(BF16)


def route_values(routes, weights, experts, slots):
    tokens = routes.shape[1]
    i = lax.broadcasted_iota(jnp.int32, (tokens, tokens), 0)
    j = lax.broadcasted_iota(jnp.int32, (tokens, tokens), 1)
    across = routes.astype(F32)
    along = weights.astype(BF16).astype(F32)
    expert = lax.broadcasted_iota(jnp.int32, (experts, tokens), 0).astype(F32)
    named = [(expert == across[k : k + 1]).astype(F32) for k in range(2)]
    earlier = mm((named[0] + named[1]).astype(BF16), (i < j).astype(BF16), None)
    row = lax.broadcasted_iota(jnp.int32, (experts * slots, tokens), 0).astype(F32)
    placing = jnp.zeros(row.shape, F32)
    weighing = jnp.zeros(row.shape, F32)
    for k in range(2):
        slot = jnp.sum(named[k] * earlier, axis=0, keepdims=True)
        match = row == across[k : k + 1] * slots + slot
        placing = placing + jnp.where(match, 1.0, 0.0)
        weighing = weighing + jnp.where(match, along[k : k + 1], 0.0)
    return placing.astype(BF16), weighing.astype(BF16)


def dispatch_kernel(experts, slots, core, rows, gain, routes, weights, buffer, weighing):
    placing, weigh = route_values(routes[...], weights[...], experts, slots)
    weighing[...] = weigh
    normed = norm_rows(rows[...], gain[...])
    width = normed.shape[1] // 2
    mine = jnp.where(core[0] == 0, normed[:, :width].astype(F32), normed[:, width:].astype(F32))
    buffer[...] = mm(placing, mine.astype(BF16), None).astype(BF16)


def placed(value, space):
    if isinstance(value, jax.ShapeDtypeStruct):
        return space(value.shape, value.dtype)
    return pltpu.with_memory_space_constraint(value, space)


near = lambda value: placed(value, pltpu.VMEM)
far = lambda value: placed(value, pltpu.HBM)


def call(kernel, outs, scalars, *args):
    smem = pl.BlockSpec(memory_space=pltpu.SMEM)
    vmem = pl.BlockSpec(memory_space=pltpu.VMEM)
    return pl.pallas_call(
        kernel,
        out_shape=outs,
        in_specs=[smem] * len(scalars) + [vmem] * len(args),
        out_specs=jax.tree.map(lambda _: vmem, outs),
        compiler_params=pltpu.CompilerParams(vmem_limit_bytes=LIMIT),
    )(*scalars, *args)


def shards(
    mixer_input_rows,
    mix_gain,
    w_recept,
    w_key,
    w_value,
    lowered_map_factor,
    decay_up,
    rate_up,
    decay_base,
    rate_base,
    decay_shift,
    out_gain,
    w_output,
    moe_rows,
    moe_gain,
    routes,
    route_weight,
    exp_gate,
    exp_up,
    exp_down,
):
    experts, tp = (lax.axis_size("ep"), lax.axis_size("tp"))
    place, lane = (lax.axis_index("ep"), lax.axis_index("tp"))
    core = lane & 1
    chips = tp // 2
    across = 4
    runs = experts // across
    run = place // across
    trade = lambda value, bit: lax.ppermute(value, "ep", [(k, k ^ bit) for k in range(experts)])
    upper = lambda bit: scalar((place & bit) != 0)
    swap = [(k, k ^ 1) for k in range(tp)]
    tokens, model = moe_rows.shape
    slots = 4 * tokens // experts
    half = model // 2
    width = w_key.shape[1]
    piece = model // tp
    scalar = lambda v: v.astype(jnp.int32).reshape(1)
    shape = jax.ShapeDtypeStruct

    buffer, weighing = call(
        functools.partial(dispatch_kernel, experts, slots),
        (shape((experts * slots, half), BF16), far(shape((experts * slots, tokens), BF16))),
        (scalar(core),),
        far(moe_rows),
        far(moe_gain.reshape(1, -1)),
        far(routes.T),
        far(route_weight.T),
    )
    arrived = lax.all_to_all(
        buffer.reshape(experts, slots, half), "ep", split_axis=0, concat_axis=0, tiled=True
    ).reshape(experts * slots, half)

    reads = far(shape((tokens, 2 * width), F32))
    wide = far(shape((width, 2 * width), F32))
    reads_f, reads_b, both = call(
        mixer_kernel,
        (reads, reads, near(shape((2 * width, 2 * width), BF16))),
        (),
        far(mixer_input_rows),
        far(mix_gain.reshape(1, -1)),
        far(w_recept.T),
        far(w_key.T),
        far(w_value.T),
        far(lowered_map_factor.T),
        far(decay_up),
        far(rate_up),
        far(decay_base.reshape(1, -1)),
        far(rate_base.reshape(1, -1)),
        far(decay_shift.T),
    )

    theirs = trade(both, 1)
    total, before, after = call(
        first_kernel,
        (near(shape((2 * width, 2 * width), BF16)), wide, wide),
        (upper(1),),
        near(both),
        near(theirs),
    )
    theirs = trade(total, 2)
    sent, before, after = call(
        send_kernel,
        (near(shape((runs, width, 2 * width), BF16)), wide, wide),
        (upper(2), scalar(run)),
        near(total),
        near(theirs),
        far(before),
        far(after),
    )

    inner = exp_gate.shape[2]
    columns = far(shape((inner, half), BF16))
    gate, down_own, down_away = call(
        functools.partial(sort_kernel, piece),
        (near(shape((model, inner), BF16)), columns, columns),
        (scalar(core),),
        far(exp_gate[0]),
        far(exp_down[0]),
    )
    down_other = lax.ppermute(down_away, "tp", swap)

    arrived, sent, down_other = lax.optimization_barrier((arrived, sent, down_other))

    carried = lax.all_to_all(
        sent,
        "ep",
        split_axis=0,
        concat_axis=0,
        tiled=True,
        axis_index_groups=[[z * across + x for z in range(runs)] for x in range(across)],
    )

    swapped = lax.ppermute(arrived, "tp", swap)
    hidden = call(
        expert_kernel,
        near(shape((experts * slots, inner), BF16)),
        (scalar(core),),
        near(arrived),
        near(swapped),
        near(gate),
        near(exp_up[0]),
    )
    landed = lax.ppermute(hidden, "tp", swap)
    paired = call(
        pair_kernel,
        near(shape((experts * slots, half), BF16)),
        (),
        near(hidden),
        near(landed),
        near(down_own),
        near(down_other),
    )

    returned = lax.all_to_all(
        paired.reshape(experts, slots, half), "ep", split_axis=0, concat_axis=0, tiled=True
    ).reshape(experts * slots, half)

    shares = shape((chips, tokens // tp, model), BF16)
    own_rows, away_rows = call(
        output_kernel,
        (near(shares), near(shares)),
        (scalar(run), scalar(core)),
        near(carried),
        far(before),
        far(after),
        far(reads_f),
        far(reads_b),
        far(out_gain.reshape(1, -1)),
        far(w_output),
    )
    landed_rows = lax.ppermute(away_rows, "tp", swap)

    parts = call(
        combine_kernel,
        near(shape((chips, 2 * tokens, piece), BF16)),
        (),
        near(returned),
        far(weighing),
        near(own_rows),
        near(landed_rows),
    )
    parts = lax.all_to_all(
        parts,
        "tp",
        split_axis=0,
        concat_axis=0,
        tiled=True,
        axis_index_groups=[[2 * y + c for y in range(chips)] for c in range(2)],
    )
    mix_out, moe_out = call(
        finish_kernel,
        (shape((tokens // tp, model), BF16), shape((tokens, piece), BF16)),
        (),
        near(parts),
    )
    return (mix_out, moe_out)


def solution(mesh):
    return jax.shard_map(
        shards,
        mesh=mesh,
        in_specs=(
            P("ep", None),
            P(),
            P(None, "tp"),
            P(None, "tp"),
            P(None, "tp"),
            P(),
            P(None, "tp"),
            P(None, "tp"),
            P("tp"),
            P("tp"),
            P("ep", "tp"),
            P("tp"),
            P("tp", None),
            P("ep", None),
            P(),
            P("ep", None),
            P("ep", None),
            P("ep", None, "tp"),
            P("ep", None, "tp"),
            P("ep", "tp", None),
        ),
        out_specs=(P(("ep", "tp"), None), P("ep", "tp")),
        check_vma=False,
    )
```

```python
import functools
import math

import jax
import jax.numpy as jnp
from jax import lax
from jax.experimental import pallas as pl
from jax.experimental.pallas import tpu as pltpu
from jax.sharding import PartitionSpec as P


DECAY_SCALE = math.exp(-0.5)
HIGH = lax.Precision.HIGH
F32 = jnp.float32
BF16 = jnp.bfloat16
BLOCK = 256
LIMIT = 16 * 1024 * 1024


def mm(a, b, precision=HIGH):
    return lax.dot_general(
        a, b, (((1,), (0,)), ((), ())), precision=precision, preferred_element_type=F32
    )


def mm_nt(a, b, precision=HIGH):
    return lax.dot_general(
        a, b, (((1,), (1,)), ((), ())), precision=precision, preferred_element_type=F32
    )


def mm_tn(a, b, precision=HIGH):
    return lax.dot_general(
        a, b, (((0,), (0,)), ((), ())), precision=precision, preferred_element_type=F32
    )


def norm_rows(rows, gain):
    entries = rows.astype(F32)
    factor = lax.rsqrt(jnp.mean(entries * entries, axis=-1, keepdims=True) + 1e-06)
    return (entries * factor * gain).astype(BF16)


def block_totals(log_decay, unit, rate, key, value, recept, reverse):
    tokens, width = log_decay.shape
    half = tokens // 2
    i = lax.broadcasted_iota(jnp.int32, (tokens, tokens), 0)
    j = lax.broadcasted_iota(jnp.int32, (tokens, tokens), 1)
    upto = (j >= i) if reverse else (j <= i)
    before = (j > i) if reverse else (j < i)
    same = (i // half) == (j // half)
    cum = mm(upto.astype(F32), log_decay)
    exc = cum - log_decay
    row = lax.broadcasted_iota(jnp.int32, (tokens, width), 0)
    if reverse:
        total = cum[:1]
        edge = cum[half : half + 1]
        first = row >= half
        mid_low, mid_high = (half // 2, half + half // 2)
    else:
        total = cum[tokens - 1 :]
        edge = cum[half - 1 : half]
        first = row < half
        mid_low, mid_high = (half // 2 - 1, half + half // 2 - 1)
    ref = jnp.where(row < half, cum[mid_low : mid_low + 1], cum[mid_high : mid_high + 1])
    learned = unit * rate
    down = jnp.exp(ref - cum)
    near_left = jnp.concatenate([unit * jnp.exp(exc - ref), recept * jnp.exp(cum - ref)], axis=0)
    near_right = jnp.concatenate([learned * down, key * down], axis=0)
    gone = jnp.full_like(cum, -1e30)
    far_down = jnp.exp(jnp.where(first, edge - cum, gone))
    far_left = jnp.concatenate(
        [
            unit * jnp.exp(jnp.where(first, gone, exc - edge)),
            recept * jnp.exp(jnp.where(first, gone, cum - edge)),
        ],
        axis=0,
    )
    far_right = jnp.concatenate([learned * far_down, key * far_down], axis=0)
    near = mm_nt(near_left, near_right)
    far = mm_nt(far_left, far_right)

    def part(up, left, mask):
        rows = slice(0, tokens) if up else slice(tokens, 2 * tokens)
        cols = slice(0, tokens) if left else slice(tokens, 2 * tokens)
        return jnp.where(mask, jnp.where(same, near[rows, cols], far[rows, cols]), 0.0)

    lower = part(True, True, before)
    unit_key = part(True, False, before)
    read_rank = part(False, True, upto)
    read_key = part(False, False, upto)
    eye = (i == j).astype(F32)
    inverse = eye - jnp.where((i // 2) == (j // 2), lower, 0.0)
    size = 2
    while size < half:
        link = jnp.where(((i // (2 * size)) == (j // (2 * size))) & ((i // size) != (j // size)), lower, 0.0)
        inverse = inverse - mm(inverse, mm(link, inverse))
        size *= 2
    written = mm(jnp.concatenate([unit_key, read_key], axis=0), value)
    right = jnp.concatenate([unit * jnp.exp(exc), written[:tokens]], axis=1)
    solved = mm(inverse, right)
    cross = jnp.where(same, 0.0, lower)
    solved = solved - mm(inverse, mm(cross, solved))
    reads = jnp.concatenate([recept * jnp.exp(cum), written[tokens:]], axis=1) - mm(read_rank, solved)
    tail = jnp.exp(total - cum)
    ki = lax.broadcasted_iota(jnp.int32, (width, width), 0)
    kj = lax.broadcasted_iota(jnp.int32, (width, width), 1)
    diag = jnp.where(ki == kj, jnp.broadcast_to(jnp.exp(total), (width, width)), 0.0)
    maps = jnp.concatenate([diag, mm_tn(key * tail, value)], axis=1) - mm_tn(learned * tail, solved)
    return reads, maps


def mixer_values(rows, gain, w_recept, w_key, w_value, w_low, decay_up, rate_up, decay_base, rate_base, shift):
    normed = norm_rows(rows, gain)

    def project(weight):
        return mm_nt(normed, weight, None).astype(BF16).astype(F32)

    recept, key, value = (project(w_recept), project(w_key), project(w_value))
    low = jnp.tanh(mm_nt(normed, w_low, None)).astype(BF16)
    tokens = rows.shape[0]
    i = lax.broadcasted_iota(jnp.int32, (tokens, tokens), 0)
    j = lax.broadcasted_iota(jnp.int32, (tokens, tokens), 1)
    shift = jnp.sum(jnp.where(i == j, shift, 0.0), axis=1, keepdims=True)
    log_decay = -DECAY_SCALE * jax.nn.sigmoid(decay_base + mm(low, decay_up, None)) + shift
    rate = jax.nn.sigmoid(rate_base + mm(low, rate_up, None))
    unit = key * lax.rsqrt(jnp.sum(key * key, axis=-1, keepdims=True) + 1e-06)
    ahead = block_totals(log_decay, unit, rate, key, value, recept, False)
    back = block_totals(log_decay, unit, rate, key, value, recept, True)
    return ahead, back


def mixer_kernel(*refs):
    ins, (reads_f, reads_b, maps) = refs[:11], refs[11:]
    ahead, back = mixer_values(*[ref[...] for ref in ins])
    reads_f[...] = ahead[0]
    reads_b[...] = back[0]
    width = ahead[1].shape[0]
    maps[:width] = ahead[1].astype(BF16)
    maps[width:] = back[1].astype(BF16)


def with_identity(maps):
    width = maps.shape[0]
    r = lax.broadcasted_iota(jnp.int32, maps.shape, 0)
    c = lax.broadcasted_iota(jnp.int32, maps.shape, 1)
    return jnp.concatenate([maps, (c == r + width).astype(maps.dtype)], axis=0)


def chained(blocks, reverse):
    level = blocks
    while len(level) > 1:
        last = len(level) == 2
        joined = []
        for k in range(0, len(level), 2):
            early, late = (level[k + 1], level[k]) if reverse else (level[k], level[k + 1])
            product = mm(late, with_identity(early), None)
            joined.append(product if last else product.astype(BF16))
        level = joined
    return level[0]


def plain_like(maps):
    r = lax.broadcasted_iota(jnp.int32, maps.shape, 0)
    c = lax.broadcasted_iota(jnp.int32, maps.shape, 1)
    return (r == c).astype(F32)


def kept(maps, use, plain):
    return jnp.where(use, maps.astype(F32), plain).astype(BF16)


def composed(late, early):
    return mm(late.astype(BF16), with_identity(early.astype(BF16)), None)


def joined(high, mine, theirs, before, after):
    width = before.shape[0]
    r = lax.broadcasted_iota(jnp.int32, before.shape, 0)
    c = lax.broadcasted_iota(jnp.int32, before.shape, 1)
    plain = (r == c).astype(F32)
    mine_f, mine_b = (mine[:width].astype(F32), mine[width:].astype(F32))
    their_f, their_b = (theirs[:width].astype(F32), theirs[width:].astype(F32))
    before = composed(before, jnp.where(high, their_f, plain))
    after = composed(after, jnp.where(high, plain, their_b))
    ahead = composed(jnp.where(high, mine_f, their_f), jnp.where(high, their_f, mine_f))
    back = composed(jnp.where(high, their_b, mine_b), jnp.where(high, mine_b, their_b))
    return ahead, back, before, after


def first_kernel(high, mine, theirs, total, before, after):
    width = before.shape[0]
    r = lax.broadcasted_iota(jnp.int32, before.shape, 0)
    c = lax.broadcasted_iota(jnp.int32, before.shape, 1)
    plain = (r == c).astype(F32)
    ahead, back, before[...], after[...] = joined(high[0] != 0, mine[...], theirs[...], plain, plain)
    total[:width] = ahead.astype(BF16)
    total[width:] = back.astype(BF16)


def send_kernel(high, run, mine, theirs, before_in, after_in, sent, before, after):
    ahead, back, before[...], after[...] = joined(
        high[0] != 0, mine[...], theirs[...], before_in[...], after_in[...]
    )
    for k in range(sent.shape[0]):
        sent[k] = jnp.where(k > run[0], ahead, back).astype(BF16)


def output_kernel(
    run, core, arrived, before, after, reads_f, reads_b, gain, w_output, own, away
):
    count, width = arrived.shape[0], before.shape[0]
    plain = plain_like(arrived[0])
    ahead = chained([kept(arrived[k], k < run[0], plain) for k in range(count)], False)
    back = chained([kept(arrived[k], k > run[0], plain) for k in range(count)], True)
    ahead = mm(before[...], with_identity(ahead))
    back = mm(after[...], with_identity(back))
    mixed = mm(reads_f[...], with_identity(ahead)) + mm(reads_b[...], with_identity(back))
    mixed = mixed[:, width:]
    centre = mixed - jnp.mean(mixed, axis=-1, keepdims=True)
    scaled = centre * lax.rsqrt(jnp.mean(centre * centre, axis=-1, keepdims=True) + 1e-05)
    split = (scaled * gain[...]).reshape(own.shape[0], 2, -1, width)
    for out, use in ((own, core[0] == 0), (away, core[0] != 0)):
        rows = jnp.where(use, split[:, 0], split[:, 1]).reshape(-1, width)
        out[...] = mm(rows.astype(BF16), w_output[...], None).astype(BF16).reshape(out.shape)


def sort_kernel(width, core, gate, down, held, own, away):
    held[...] = gate[...]
    for out, parity in ((own, core[0]), (away, 1 - core[0])):
        for y in range(out.shape[1] // width):
            columns = pl.ds(pl.multiple_of((2 * y + parity) * width, width), width)
            out[:, y * width : (y + 1) * width] = down[:, columns]


def expert_kernel(core, arrived, swapped, gate, up, hidden):
    half = arrived.shape[1]
    at = core[0]
    near_rows = pl.ds(pl.multiple_of(at * half, half), half)
    far_rows = pl.ds(pl.multiple_of((1 - at) * half, half), half)
    pairs = [(arrived[...], near_rows), (swapped[...], far_rows)]
    gated = sum(mm(value, gate[where, :], None) for value, where in pairs)
    raised = sum(mm(value, up[where, :], None) for value, where in pairs)
    hidden[...] = (gated / (1.0 + jnp.exp(-gated)) * raised).astype(BF16)


def pair_kernel(hidden, landed, own, other, out):
    rows = jnp.concatenate([hidden[...], landed[...]], axis=1)
    for k in range(0, out.shape[1], BLOCK):
        columns = slice(k, k + BLOCK)
        weight = jnp.concatenate([own[:, columns], other[:, columns]], axis=0)
        out[:, columns] = mm(rows, weight, None).astype(BF16)


def halve_kernel(bit, mine, landed, keep, send):
    for k in range(keep.shape[0]):
        total = [(mine[2 * k + m].astype(F32) + landed[2 * k + m].astype(F32)) for m in range(2)]
        keep[k] = jnp.where(bit[0] != 0, total[1], total[0]).astype(BF16)
        send[k] = jnp.where(bit[0] != 0, total[0], total[1]).astype(BF16)


def combine_kernel(returned, weighing, out):
    width = out.shape[2]
    weighed = mm_tn(weighing[...], returned[...], None).astype(BF16)
    for y in range(out.shape[0]):
        out[y] = weighed[:, y * width : (y + 1) * width]


def finish_kernel(shares, keep, landed, mixed, moe):
    total = shares[0].astype(F32)
    for y in range(1, shares.shape[0]):
        total = total + shares[y].astype(F32)
    moe[...] = total.astype(BF16)
    mixed[...] = (keep[0].astype(F32) + landed[0].astype(F32)).astype(BF16)


def route_values(routes, weights, experts, slots):
    tokens = routes.shape[1]
    i = lax.broadcasted_iota(jnp.int32, (tokens, tokens), 0)
    j = lax.broadcasted_iota(jnp.int32, (tokens, tokens), 1)
    across = routes.astype(F32)
    along = weights.astype(BF16).astype(F32)
    expert = lax.broadcasted_iota(jnp.int32, (experts, tokens), 0).astype(F32)
    named = [(expert == across[k : k + 1]).astype(F32) for k in range(2)]
    earlier = mm((named[0] + named[1]).astype(BF16), (i < j).astype(BF16), None)
    row = lax.broadcasted_iota(jnp.int32, (experts * slots, tokens), 0).astype(F32)
    placing = jnp.zeros(row.shape, F32)
    weighing = jnp.zeros(row.shape, F32)
    for k in range(2):
        slot = jnp.sum(named[k] * earlier, axis=0, keepdims=True)
        match = row == across[k : k + 1] * slots + slot
        placing = placing + jnp.where(match, 1.0, 0.0)
        weighing = weighing + jnp.where(match, along[k : k + 1], 0.0)
    return placing.astype(BF16), weighing.astype(BF16)


def dispatch_kernel(experts, slots, core, rows, gain, routes, weights, buffer, weighing):
    placing, weigh = route_values(routes[...], weights[...], experts, slots)
    weighing[...] = weigh
    normed = norm_rows(rows[...], gain[...])
    width = normed.shape[1] // 2
    mine = jnp.where(core[0] == 0, normed[:, :width].astype(F32), normed[:, width:].astype(F32))
    buffer[...] = mm(placing, mine.astype(BF16), None).astype(BF16)


def placed(value, space):
    if isinstance(value, jax.ShapeDtypeStruct):
        return space(value.shape, value.dtype)
    return pltpu.with_memory_space_constraint(value, space)


near = lambda value: placed(value, pltpu.VMEM)
far = lambda value: placed(value, pltpu.HBM)


def call(kernel, outs, scalars, *args):
    smem = pl.BlockSpec(memory_space=pltpu.SMEM)
    vmem = pl.BlockSpec(memory_space=pltpu.VMEM)
    return pl.pallas_call(
        kernel,
        out_shape=outs,
        in_specs=[smem] * len(scalars) + [vmem] * len(args),
        out_specs=jax.tree.map(lambda _: vmem, outs),
        compiler_params=pltpu.CompilerParams(vmem_limit_bytes=LIMIT),
    )(*scalars, *args)


def shards(
    mixer_input_rows,
    mix_gain,
    w_recept,
    w_key,
    w_value,
    lowered_map_factor,
    decay_up,
    rate_up,
    decay_base,
    rate_base,
    decay_shift,
    out_gain,
    w_output,
    moe_rows,
    moe_gain,
    routes,
    route_weight,
    exp_gate,
    exp_up,
    exp_down,
):
    experts, tp = (lax.axis_size("ep"), lax.axis_size("tp"))
    place, lane = (lax.axis_index("ep"), lax.axis_index("tp"))
    core, chip = (lane & 1, lane >> 1)
    chips = tp // 2
    across = 4
    runs = experts // across
    run = place // across
    trade = lambda value, bit: lax.ppermute(value, "ep", [(k, k ^ bit) for k in range(experts)])
    upper = lambda bit: scalar((place & bit) != 0)
    swap = [(k, k ^ 1) for k in range(tp)]
    tokens, model = moe_rows.shape
    slots = 4 * tokens // experts
    half = model // 2
    width = w_key.shape[1]
    piece = model // tp
    scalar = lambda v: v.astype(jnp.int32).reshape(1)
    shape = jax.ShapeDtypeStruct

    buffer, weighing = call(
        functools.partial(dispatch_kernel, experts, slots),
        (shape((experts * slots, half), BF16), far(shape((experts * slots, tokens), BF16))),
        (scalar(core),),
        far(moe_rows),
        far(moe_gain.reshape(1, -1)),
        far(routes.T),
        far(route_weight.T),
    )
    arrived = lax.all_to_all(
        buffer.reshape(experts, slots, half), "ep", split_axis=0, concat_axis=0, tiled=True
    ).reshape(experts * slots, half)

    reads = far(shape((tokens, 2 * width), F32))
    wide = far(shape((width, 2 * width), F32))
    reads_f, reads_b, both = call(
        mixer_kernel,
        (reads, reads, near(shape((2 * width, 2 * width), BF16))),
        (),
        far(mixer_input_rows),
        far(mix_gain.reshape(1, -1)),
        far(w_recept.T),
        far(w_key.T),
        far(w_value.T),
        far(lowered_map_factor.T),
        far(decay_up),
        far(rate_up),
        far(decay_base.reshape(1, -1)),
        far(rate_base.reshape(1, -1)),
        far(decay_shift.T),
    )

    theirs = trade(both, 1)
    total, before, after = call(
        first_kernel,
        (near(shape((2 * width, 2 * width), BF16)), wide, wide),
        (upper(1),),
        near(both),
        near(theirs),
    )
    theirs = trade(total, 2)
    sent, before, after = call(
        send_kernel,
        (near(shape((runs, width, 2 * width), BF16)), wide, wide),
        (upper(2), scalar(run)),
        near(total),
        near(theirs),
        far(before),
        far(after),
    )

    inner = exp_gate.shape[2]
    columns = far(shape((inner, half), BF16))
    gate, down_own, down_away = call(
        functools.partial(sort_kernel, piece),
        (near(shape((model, inner), BF16)), columns, columns),
        (scalar(core),),
        far(exp_gate[0]),
        far(exp_down[0]),
    )
    down_other = lax.ppermute(down_away, "tp", swap)

    arrived, sent, down_other = lax.optimization_barrier((arrived, sent, down_other))

    carried = lax.all_to_all(
        sent,
        "ep",
        split_axis=0,
        concat_axis=0,
        tiled=True,
        axis_index_groups=[[z * across + x for z in range(runs)] for x in range(across)],
    )

    swapped = lax.ppermute(arrived, "tp", swap)
    hidden = call(
        expert_kernel,
        near(shape((experts * slots, inner), BF16)),
        (scalar(core),),
        near(arrived),
        near(swapped),
        near(gate),
        near(exp_up[0]),
    )
    landed = lax.ppermute(hidden, "tp", swap)
    paired = call(
        pair_kernel,
        near(shape((experts * slots, half), BF16)),
        (),
        near(hidden),
        near(landed),
        near(down_own),
        near(down_other),
    )

    returned = lax.all_to_all(
        paired.reshape(experts, slots, half), "ep", split_axis=0, concat_axis=0, tiled=True
    ).reshape(experts * slots, half)

    shares = shape((chips, tokens // tp, model), BF16)
    own_rows, away_rows = call(
        output_kernel,
        (near(shares), near(shares)),
        (scalar(run), scalar(core)),
        near(carried),
        far(before),
        far(after),
        far(reads_f),
        far(reads_b),
        far(out_gain.reshape(1, -1)),
        far(w_output),
    )
    keep, landed = (own_rows, lax.ppermute(away_rows, "tp", swap))
    bit = 1
    while bit < chips:
        part = near(shape((keep.shape[0] // 2, tokens // tp, model), BF16))
        keep, send = call(
            halve_kernel,
            (part, part),
            (scalar((chip & bit) != 0),),
            near(keep),
            near(landed),
        )
        landed = lax.ppermute(send, "tp", [(k, k ^ (2 * bit)) for k in range(tp)])
        bit *= 2

    parts = call(
        combine_kernel,
        near(shape((chips, tokens, piece), BF16)),
        (),
        near(returned),
        far(weighing),
    )
    parts = lax.all_to_all(
        parts,
        "tp",
        split_axis=0,
        concat_axis=0,
        tiled=True,
        axis_index_groups=[[2 * y + c for y in range(chips)] for c in range(2)],
    )
    mix_out, moe_out = call(
        finish_kernel,
        (shape((tokens // tp, model), BF16), shape((tokens, piece), BF16)),
        (),
        near(parts),
        near(keep),
        near(landed),
    )
    return (mix_out, moe_out)


def solution(mesh):
    return jax.shard_map(
        shards,
        mesh=mesh,
        in_specs=(
            P("ep", None),
            P(),
            P(None, "tp"),
            P(None, "tp"),
            P(None, "tp"),
            P(),
            P(None, "tp"),
            P(None, "tp"),
            P("tp"),
            P("tp"),
            P("ep", "tp"),
            P("tp"),
            P("tp", None),
            P("ep", None),
            P(),
            P("ep", None),
            P("ep", None),
            P("ep", None, "tp"),
            P("ep", None, "tp"),
            P("ep", "tp", None),
        ),
        out_specs=(P(("ep", "tp"), None), P("ep", "tp")),
        check_vma=False,
    )
```

```python
import functools
import math

import jax
import jax.numpy as jnp
from jax import lax
from jax.experimental import pallas as pl
from jax.experimental.pallas import tpu as pltpu
from jax.sharding import PartitionSpec as P


DECAY_SCALE = math.exp(-0.5)
HIGH = lax.Precision.HIGH
F32 = jnp.float32
BF16 = jnp.bfloat16
BLOCK = 256
LIMIT = 16 * 1024 * 1024


def mm(a, b, precision=HIGH):
    return lax.dot_general(
        a, b, (((1,), (0,)), ((), ())), precision=precision, preferred_element_type=F32
    )


def mm_nt(a, b, precision=HIGH):
    return lax.dot_general(
        a, b, (((1,), (1,)), ((), ())), precision=precision, preferred_element_type=F32
    )


def mm_tn(a, b, precision=HIGH):
    return lax.dot_general(
        a, b, (((0,), (0,)), ((), ())), precision=precision, preferred_element_type=F32
    )


def norm_rows(rows, gain):
    entries = rows.astype(F32)
    factor = lax.rsqrt(jnp.mean(entries * entries, axis=-1, keepdims=True) + 1e-06)
    return (entries * factor * gain).astype(BF16)


def block_totals(log_decay, unit, rate, key, value, recept, reverse):
    tokens, width = log_decay.shape
    half = tokens // 2
    i = lax.broadcasted_iota(jnp.int32, (tokens, tokens), 0)
    j = lax.broadcasted_iota(jnp.int32, (tokens, tokens), 1)
    upto = (j >= i) if reverse else (j <= i)
    before = (j > i) if reverse else (j < i)
    same = (i // half) == (j // half)
    cum = mm(upto.astype(F32), log_decay)
    exc = cum - log_decay
    row = lax.broadcasted_iota(jnp.int32, (tokens, width), 0)
    if reverse:
        total = cum[:1]
        edge = cum[half : half + 1]
        first = row >= half
        mid_low, mid_high = (half // 2, half + half // 2)
    else:
        total = cum[tokens - 1 :]
        edge = cum[half - 1 : half]
        first = row < half
        mid_low, mid_high = (half // 2 - 1, half + half // 2 - 1)
    ref = jnp.where(row < half, cum[mid_low : mid_low + 1], cum[mid_high : mid_high + 1])
    learned = unit * rate
    down = jnp.exp(ref - cum)
    near_left = jnp.concatenate([unit * jnp.exp(exc - ref), recept * jnp.exp(cum - ref)], axis=0)
    near_right = jnp.concatenate([learned * down, key * down], axis=0)
    gone = jnp.full_like(cum, -1e30)
    far_down = jnp.exp(jnp.where(first, edge - cum, gone))
    far_left = jnp.concatenate(
        [
            unit * jnp.exp(jnp.where(first, gone, exc - edge)),
            recept * jnp.exp(jnp.where(first, gone, cum - edge)),
        ],
        axis=0,
    )
    far_right = jnp.concatenate([learned * far_down, key * far_down], axis=0)
    near = mm_nt(near_left, near_right)
    far = mm_nt(far_left, far_right)

    def part(up, left, mask):
        rows = slice(0, tokens) if up else slice(tokens, 2 * tokens)
        cols = slice(0, tokens) if left else slice(tokens, 2 * tokens)
        return jnp.where(mask, jnp.where(same, near[rows, cols], far[rows, cols]), 0.0)

    lower = part(True, True, before)
    unit_key = part(True, False, before)
    read_rank = part(False, True, upto)
    read_key = part(False, False, upto)
    eye = (i == j).astype(F32)
    inverse = eye - jnp.where((i // 2) == (j // 2), lower, 0.0)
    size = 2
    while size < half:
        link = jnp.where(((i // (2 * size)) == (j // (2 * size))) & ((i // size) != (j // size)), lower, 0.0)
        inverse = inverse - mm(inverse, mm(link, inverse))
        size *= 2
    written = mm(jnp.concatenate([unit_key, read_key], axis=0), value)
    right = jnp.concatenate([unit * jnp.exp(exc), written[:tokens]], axis=1)
    solved = mm(inverse, right)
    cross = jnp.where(same, 0.0, lower)
    solved = solved - mm(inverse, mm(cross, solved))
    reads = jnp.concatenate([recept * jnp.exp(cum), written[tokens:]], axis=1) - mm(read_rank, solved)
    tail = jnp.exp(total - cum)
    ki = lax.broadcasted_iota(jnp.int32, (width, width), 0)
    kj = lax.broadcasted_iota(jnp.int32, (width, width), 1)
    diag = jnp.where(ki == kj, jnp.broadcast_to(jnp.exp(total), (width, width)), 0.0)
    maps = jnp.concatenate([diag, mm_tn(key * tail, value)], axis=1) - mm_tn(learned * tail, solved)
    return reads, maps


def mixer_values(rows, gain, w_recept, w_key, w_value, w_low, decay_up, rate_up, decay_base, rate_base, shift):
    normed = norm_rows(rows, gain)

    def project(weight):
        return mm_nt(normed, weight, None).astype(BF16).astype(F32)

    recept, key, value = (project(w_recept), project(w_key), project(w_value))
    low = jnp.tanh(mm_nt(normed, w_low, None)).astype(BF16)
    tokens = rows.shape[0]
    i = lax.broadcasted_iota(jnp.int32, (tokens, tokens), 0)
    j = lax.broadcasted_iota(jnp.int32, (tokens, tokens), 1)
    shift = jnp.sum(jnp.where(i == j, shift, 0.0), axis=1, keepdims=True)
    log_decay = -DECAY_SCALE * jax.nn.sigmoid(decay_base + mm(low, decay_up, None)) + shift
    rate = jax.nn.sigmoid(rate_base + mm(low, rate_up, None))
    unit = key * lax.rsqrt(jnp.sum(key * key, axis=-1, keepdims=True) + 1e-06)
    ahead = block_totals(log_decay, unit, rate, key, value, recept, False)
    back = block_totals(log_decay, unit, rate, key, value, recept, True)
    return ahead, back


def mixer_kernel(*refs):
    ins, (reads_f, reads_b, maps) = refs[:11], refs[11:]
    ahead, back = mixer_values(*[ref[...] for ref in ins])
    reads_f[...] = ahead[0]
    reads_b[...] = back[0]
    width = ahead[1].shape[0]
    maps[:width] = ahead[1].astype(BF16)
    maps[width:] = back[1].astype(BF16)


def with_identity(maps):
    width = maps.shape[0]
    r = lax.broadcasted_iota(jnp.int32, maps.shape, 0)
    c = lax.broadcasted_iota(jnp.int32, maps.shape, 1)
    return jnp.concatenate([maps, (c == r + width).astype(maps.dtype)], axis=0)


def chained(blocks, reverse):
    level = blocks
    while len(level) > 1:
        last = len(level) == 2
        joined = []
        for k in range(0, len(level), 2):
            early, late = (level[k + 1], level[k]) if reverse else (level[k], level[k + 1])
            product = mm(late, with_identity(early), None)
            joined.append(product if last else product.astype(BF16))
        level = joined
    return level[0]


def plain_like(maps):
    r = lax.broadcasted_iota(jnp.int32, maps.shape, 0)
    c = lax.broadcasted_iota(jnp.int32, maps.shape, 1)
    return (r == c).astype(F32)


def kept(maps, use, plain):
    return jnp.where(use, maps.astype(F32), plain).astype(BF16)


def composed(late, early):
    return mm(late.astype(BF16), with_identity(early.astype(BF16)), None)


def joined(high, mine, theirs, before, after):
    width = before.shape[0]
    r = lax.broadcasted_iota(jnp.int32, before.shape, 0)
    c = lax.broadcasted_iota(jnp.int32, before.shape, 1)
    plain = (r == c).astype(F32)
    mine_f, mine_b = (mine[:width].astype(F32), mine[width:].astype(F32))
    their_f, their_b = (theirs[:width].astype(F32), theirs[width:].astype(F32))
    before = composed(before, jnp.where(high, their_f, plain))
    after = composed(after, jnp.where(high, plain, their_b))
    ahead = composed(jnp.where(high, mine_f, their_f), jnp.where(high, their_f, mine_f))
    back = composed(jnp.where(high, their_b, mine_b), jnp.where(high, mine_b, their_b))
    return ahead, back, before, after


def first_kernel(high, mine, theirs, total, before, after):
    width = before.shape[0]
    r = lax.broadcasted_iota(jnp.int32, before.shape, 0)
    c = lax.broadcasted_iota(jnp.int32, before.shape, 1)
    plain = (r == c).astype(F32)
    ahead, back, before[...], after[...] = joined(high[0] != 0, mine[...], theirs[...], plain, plain)
    total[:width] = ahead.astype(BF16)
    total[width:] = back.astype(BF16)


def send_kernel(high, run, mine, theirs, before_in, after_in, sent, before, after):
    ahead, back, before[...], after[...] = joined(
        high[0] != 0, mine[...], theirs[...], before_in[...], after_in[...]
    )
    for k in range(sent.shape[0]):
        sent[k] = jnp.where(k > run[0], ahead, back).astype(BF16)


def output_kernel(
    run, core, arrived, before, after, reads_f, reads_b, gain, w_output, own, away
):
    count, width = arrived.shape[0], before.shape[0]
    plain = plain_like(arrived[0])
    ahead = chained([kept(arrived[k], k < run[0], plain) for k in range(count)], False)
    back = chained([kept(arrived[k], k > run[0], plain) for k in range(count)], True)
    ahead = mm(before[...], with_identity(ahead))
    back = mm(after[...], with_identity(back))
    mixed = mm(reads_f[...], with_identity(ahead)) + mm(reads_b[...], with_identity(back))
    mixed = mixed[:, width:]
    centre = mixed - jnp.mean(mixed, axis=-1, keepdims=True)
    scaled = centre * lax.rsqrt(jnp.mean(centre * centre, axis=-1, keepdims=True) + 1e-05)
    split = (scaled * gain[...]).reshape(own.shape[0], 2, -1, width)
    for out, use in ((own, core[0] == 0), (away, core[0] != 0)):
        rows = jnp.where(use, split[:, 0], split[:, 1]).reshape(-1, width)
        out[...] = mm(rows.astype(BF16), w_output[...], None).astype(BF16).reshape(out.shape)


def sort_kernel(width, core, gate, down, held, own, away):
    held[...] = gate[...]
    for out, parity in ((own, core[0]), (away, 1 - core[0])):
        for y in range(out.shape[1] // width):
            columns = pl.ds(pl.multiple_of((2 * y + parity) * width, width), width)
            out[:, y * width : (y + 1) * width] = down[:, columns]


def expert_kernel(core, arrived, swapped, gate, up, hidden):
    half = arrived.shape[1]
    at = core[0]
    near_rows = pl.ds(pl.multiple_of(at * half, half), half)
    far_rows = pl.ds(pl.multiple_of((1 - at) * half, half), half)
    pairs = [(arrived[...], near_rows), (swapped[...], far_rows)]
    gated = sum(mm(value, gate[where, :], None) for value, where in pairs)
    raised = sum(mm(value, up[where, :], None) for value, where in pairs)
    hidden[...] = (gated / (1.0 + jnp.exp(-gated)) * raised).astype(BF16)


def pair_kernel(hidden, landed, own, other, out):
    rows = jnp.concatenate([hidden[...], landed[...]], axis=1)
    for k in range(0, out.shape[1], BLOCK):
        columns = slice(k, k + BLOCK)
        weight = jnp.concatenate([own[:, columns], other[:, columns]], axis=0)
        out[:, columns] = mm(rows, weight, None).astype(BF16)


def halve_kernel(bit, mine, landed, keep, send):
    for k in range(keep.shape[0]):
        total = [(mine[2 * k + m].astype(F32) + landed[2 * k + m].astype(F32)) for m in range(2)]
        keep[k] = jnp.where(bit[0] != 0, total[1], total[0]).astype(BF16)
        send[k] = jnp.where(bit[0] != 0, total[0], total[1]).astype(BF16)


def combine_kernel(returned, weighing, out):
    width = out.shape[2]
    weighed = mm_tn(weighing[...], returned[...], None).astype(BF16)
    for y in range(out.shape[0]):
        out[y] = weighed[:, y * width : (y + 1) * width]


def finish_kernel(shares, keep, landed, mixed, moe):
    total = shares[0].astype(F32)
    for y in range(1, shares.shape[0]):
        total = total + shares[y].astype(F32)
    moe[...] = total.astype(BF16)
    mixed[...] = (keep[0].astype(F32) + landed[0].astype(F32)).astype(BF16)


def route_values(routes, weights, experts, slots):
    tokens = routes.shape[1]
    i = lax.broadcasted_iota(jnp.int32, (tokens, tokens), 0)
    j = lax.broadcasted_iota(jnp.int32, (tokens, tokens), 1)
    across = routes.astype(F32)
    along = weights.astype(BF16).astype(F32)
    expert = lax.broadcasted_iota(jnp.int32, (experts, tokens), 0).astype(F32)
    named = [(expert == across[k : k + 1]).astype(F32) for k in range(2)]
    earlier = mm((named[0] + named[1]).astype(BF16), (i < j).astype(BF16), None)
    row = lax.broadcasted_iota(jnp.int32, (experts * slots, tokens), 0).astype(F32)
    placing = jnp.zeros(row.shape, F32)
    weighing = jnp.zeros(row.shape, F32)
    for k in range(2):
        slot = jnp.sum(named[k] * earlier, axis=0, keepdims=True)
        match = row == across[k : k + 1] * slots + slot
        placing = placing + jnp.where(match, 1.0, 0.0)
        weighing = weighing + jnp.where(match, along[k : k + 1], 0.0)
    return placing.astype(BF16), weighing.astype(BF16)


def dispatch_kernel(experts, slots, core, rows, gain, routes, weights, buffer, weighing):
    placing, weigh = route_values(routes[...], weights[...], experts, slots)
    weighing[...] = weigh
    normed = norm_rows(rows[...], gain[...])
    width = normed.shape[1] // 2
    mine = jnp.where(core[0] == 0, normed[:, :width].astype(F32), normed[:, width:].astype(F32))
    buffer[...] = mm(placing, mine.astype(BF16), None).astype(BF16)


def placed(value, space):
    if isinstance(value, jax.ShapeDtypeStruct):
        return space(value.shape, value.dtype)
    return pltpu.with_memory_space_constraint(value, space)


near = lambda value: placed(value, pltpu.VMEM)
far = lambda value: placed(value, pltpu.HBM)


def call(kernel, outs, scalars, *args):
    smem = pl.BlockSpec(memory_space=pltpu.SMEM)
    vmem = pl.BlockSpec(memory_space=pltpu.VMEM)
    return pl.pallas_call(
        kernel,
        out_shape=outs,
        in_specs=[smem] * len(scalars) + [vmem] * len(args),
        out_specs=jax.tree.map(lambda _: vmem, outs),
        compiler_params=pltpu.CompilerParams(vmem_limit_bytes=LIMIT),
    )(*scalars, *args)


def shards(
    mixer_input_rows,
    mix_gain,
    w_recept,
    w_key,
    w_value,
    lowered_map_factor,
    decay_up,
    rate_up,
    decay_base,
    rate_base,
    decay_shift,
    out_gain,
    w_output,
    moe_rows,
    moe_gain,
    routes,
    route_weight,
    exp_gate,
    exp_up,
    exp_down,
):
    experts, tp = (lax.axis_size("ep"), lax.axis_size("tp"))
    place, lane = (lax.axis_index("ep"), lax.axis_index("tp"))
    core, chip = (lane & 1, lane >> 1)
    chips = tp // 2
    across = 4
    runs = experts // across
    run = place // across
    trade = lambda value, bit: lax.ppermute(value, "ep", [(k, k ^ bit) for k in range(experts)])
    upper = lambda bit: scalar((place & bit) != 0)
    swap = [(k, k ^ 1) for k in range(tp)]
    tokens, model = moe_rows.shape
    slots = 4 * tokens // experts
    half = model // 2
    width = w_key.shape[1]
    piece = model // tp
    scalar = lambda v: v.astype(jnp.int32).reshape(1)
    shape = jax.ShapeDtypeStruct

    buffer, weighing = call(
        functools.partial(dispatch_kernel, experts, slots),
        (shape((experts * slots, half), BF16), near(shape((experts * slots, tokens), BF16))),
        (scalar(core),),
        far(moe_rows),
        far(moe_gain.reshape(1, -1)),
        far(routes.T),
        far(route_weight.T),
    )
    arrived = lax.all_to_all(
        buffer.reshape(experts, slots, half), "ep", split_axis=0, concat_axis=0, tiled=True
    ).reshape(experts * slots, half)

    reads = far(shape((tokens, 2 * width), F32))
    wide = far(shape((width, 2 * width), F32))
    reads_f, reads_b, both = call(
        mixer_kernel,
        (reads, reads, near(shape((2 * width, 2 * width), BF16))),
        (),
        far(mixer_input_rows),
        far(mix_gain.reshape(1, -1)),
        far(w_recept.T),
        far(w_key.T),
        far(w_value.T),
        far(lowered_map_factor.T),
        far(decay_up),
        far(rate_up),
        far(decay_base.reshape(1, -1)),
        far(rate_base.reshape(1, -1)),
        far(decay_shift.T),
    )

    theirs = trade(both, 1)
    total, before, after = call(
        first_kernel,
        (near(shape((2 * width, 2 * width), BF16)), wide, wide),
        (upper(1),),
        near(both),
        near(theirs),
    )
    theirs = trade(total, 2)
    sent, before, after = call(
        send_kernel,
        (near(shape((runs, width, 2 * width), BF16)), wide, wide),
        (upper(2), scalar(run)),
        near(total),
        near(theirs),
        far(before),
        far(after),
    )

    inner = exp_gate.shape[2]
    columns = far(shape((inner, half), BF16))
    gate, down_own, down_away = call(
        functools.partial(sort_kernel, piece),
        (near(shape((model, inner), BF16)), columns, columns),
        (scalar(core),),
        far(exp_gate[0]),
        far(exp_down[0]),
    )
    down_other = lax.ppermute(down_away, "tp", swap)

    arrived, sent, down_other = lax.optimization_barrier((arrived, sent, down_other))

    carried = lax.all_to_all(
        sent,
        "ep",
        split_axis=0,
        concat_axis=0,
        tiled=True,
        axis_index_groups=[[z * across + x for z in range(runs)] for x in range(across)],
    )

    swapped = lax.ppermute(arrived, "tp", swap)
    hidden = call(
        expert_kernel,
        near(shape((experts * slots, inner), BF16)),
        (scalar(core),),
        near(arrived),
        near(swapped),
        near(gate),
        near(exp_up[0]),
    )
    landed = lax.ppermute(hidden, "tp", swap)
    paired = call(
        pair_kernel,
        near(shape((experts * slots, half), BF16)),
        (),
        near(hidden),
        near(landed),
        near(down_own),
        near(down_other),
    )

    returned = lax.all_to_all(
        paired.reshape(experts, slots, half), "ep", split_axis=0, concat_axis=0, tiled=True
    ).reshape(experts * slots, half)

    shares = shape((chips, tokens // tp, model), BF16)
    own_rows, away_rows = call(
        output_kernel,
        (near(shares), near(shares)),
        (scalar(run), scalar(core)),
        near(carried),
        far(before),
        far(after),
        far(reads_f),
        far(reads_b),
        far(out_gain.reshape(1, -1)),
        near(w_output),
    )
    keep, landed = (own_rows, lax.ppermute(away_rows, "tp", swap))
    bit = 1
    while bit < chips:
        part = near(shape((keep.shape[0] // 2, tokens // tp, model), BF16))
        keep, send = call(
            halve_kernel,
            (part, part),
            (scalar((chip & bit) != 0),),
            near(keep),
            near(landed),
        )
        landed = lax.ppermute(send, "tp", [(k, k ^ (2 * bit)) for k in range(tp)])
        bit *= 2

    parts = call(
        combine_kernel,
        near(shape((chips, tokens, piece), BF16)),
        (),
        near(returned),
        near(weighing),
    )
    parts = lax.all_to_all(
        parts,
        "tp",
        split_axis=0,
        concat_axis=0,
        tiled=True,
        axis_index_groups=[[2 * y + c for y in range(chips)] for c in range(2)],
    )
    mix_out, moe_out = call(
        finish_kernel,
        (shape((tokens // tp, model), BF16), shape((tokens, piece), BF16)),
        (),
        near(parts),
        near(keep),
        near(landed),
    )
    return (mix_out, moe_out)


def solution(mesh):
    return jax.shard_map(
        shards,
        mesh=mesh,
        in_specs=(
            P("ep", None),
            P(),
            P(None, "tp"),
            P(None, "tp"),
            P(None, "tp"),
            P(),
            P(None, "tp"),
            P(None, "tp"),
            P("tp"),
            P("tp"),
            P("ep", "tp"),
            P("tp"),
            P("tp", None),
            P("ep", None),
            P(),
            P("ep", None),
            P("ep", None),
            P("ep", None, "tp"),
            P("ep", None, "tp"),
            P("ep", "tp", None),
        ),
        out_specs=(P(("ep", "tp"), None), P("ep", "tp")),
        check_vma=False,
    )
```
